512 devices in a mesh: ep: 128 (over z, y, core), tp: 4 (over x).
Axes of the slice: x: 4, y: 8, z: 8, core: 2. Of those that a mesh axis runs over, the one named last changes fastest.
Arguments:
- tokens: bfloat16 [2048, 1024], P('ep', 'tp'), may hold values from -12 to 12
- input_window: bfloat16 [2048, 3, 512], P('ep', None, 'tp'), may hold values from -6 to 6
- write_window: bfloat16 [2048, 3, 256], P('ep', None, 'tp'), may hold values from -6 to 6
- read_window: bfloat16 [2048, 3, 256], P('ep', None, 'tp'), may hold values from -6 to 6
- ssm_state: float32 [2048, 8, 64, 64], P('ep', 'tp'), may hold values from -6 to 6
- norm_gain: bfloat16 [1024], replicated, may hold values from 0.099609375 to 1.8984375
- proj_gate: bfloat16 [1024, 512], P(None, 'tp'), may hold values from -0.1875 to 0.1875
- proj_input: bfloat16 [1024, 512], P(None, 'tp'), may hold values from -0.1875 to 0.1875
- proj_write: bfloat16 [1024, 256], P(None, 'tp'), may hold values from -0.1875 to 0.1875
- proj_read: bfloat16 [1024, 256], P(None, 'tp'), may hold values from -0.1875 to 0.1875
- proj_step: bfloat16 [1024, 8], replicated, may hold values from -0.1875 to 0.1875
- taps_input: bfloat16 [4, 512], P(None, 'tp'), may hold values from -3 to 3
- taps_write: bfloat16 [4, 256], P(None, 'tp'), may hold values from -3 to 3
- taps_read: bfloat16 [4, 256], P(None, 'tp'), may hold values from -3 to 3
- step_bias: float32 [8], replicated, may hold values from -2.5 to 0.5
- decay_rate: float32 [8], replicated, may hold values from 0.02 to 2
- skip_gain: float32 [8], replicated, may hold values from 0.1 to 1.9
- out_gain: bfloat16 [512], P('tp'), may hold values from 0.099609375 to 1.8984375
- proj_out: bfloat16 [512, 1024], P('tp'), may hold values from -0.25 to 0.25
- ffn_gain: bfloat16 [1024], replicated, may hold values from 0.099609375 to 1.8984375
- expert_ids: int32 [2048, 6], P('ep'), may hold values from 0 to 127, all different within a row; in each aligned block of 16 rows (0 to 15, 16 to 31, ...) at most 2 rows name the same one
- expert_weights: float32 [2048, 6], P('ep'), may hold values from 0.05 to 1
- expert_gate: bfloat16 [128, 1024, 512], P('ep', None, 'tp'), may hold values from -0.1875 to 0.1875
- expert_up: bfloat16 [128, 1024, 512], P('ep', None, 'tp'), may hold values from -0.1875 to 0.1875
- expert_down: bfloat16 [128, 512, 1024], P('ep', 'tp'), may hold values from -0.25 to 0.25
- dense_gate: bfloat16 [1024, 1024], P(None, 'tp'), may hold values from -0.1875 to 0.1875
- dense_up: bfloat16 [1024, 1024], P(None, 'tp'), may hold values from -0.1875 to 0.1875
- dense_down: bfloat16 [1024, 1024], P(None, 'tp'), may hold values from -0.5 to 0.5
- branch_gate: bfloat16 [1024], replicated, may hold values from -0.1875 to 0.1875
Outputs:
- new_hidden: bfloat16 [2048, 1024], P('ep', 'tp')
- new_state: float32 [2048, 8, 64, 64], P('ep', 'tp')
- new_input_window: bfloat16 [2048, 3, 512], P('ep', None, 'tp')
- new_write_window: bfloat16 [2048, 3, 256], P('ep', None, 'tp')
- new_read_window: bfloat16 [2048, 3, 256], P('ep', None, 'tp')
The draws below stay inside these ranges and needn't reach their ends.
Inputs may be any that keep to these rules, and one draw needn't show every extreme that they name: `expert_ids`: each row names 6 different experts. Among the 16 rows of one index of ep no expert is named more than 2 times, and in some aligned block an expert is named exactly 2 times.
All inputs are finite; a program needn't handle non-finite values.
Results may differ from the reference program's by a relative error of at most 0.018.
Values may be sent and summed in bfloat16 or wider, within the bound.
No kernel may reach another device: no remote copies, remote signals or barrier semaphores. Data moves between devices by JAX's collectives and lax.ppermute only.
A program may use at most 64 MiB of HBM per device.

```python
import math
import jax
import jax.numpy as jnp
import numpy as np
from jax import lax

D = 1024
HEADS = 8
HEAD_DIM = 64
STATE = 64
BC_GROUPS = 4
CONV = 4
EXP_FF = 512
TOPK = 6
DENSE_FF = 1024
SEQ_DEV = 16
BATCH = 2048
EXPERTS = 128
CAP = 2
INNER = 512
LATENT = 256
FF_DEV = 128
N_EP = 128
N_TP = 4


def draw_tokens(key, part):
    key_main = jax.random.fold_in(jax.random.fold_in(key, 11), 0)
    columns = 0.5 * jnp.exp(jnp.log(4.0) * jnp.arange(D, dtype=jnp.float32) / (D - 1))
    values = jax.random.normal(key_main, (BATCH, D), jnp.float32) * columns
    return jnp.clip(values, -12.0, 12.0).astype(jnp.bfloat16)


def block_scale(stream_key, shape, pieces, low, largest):
    loudness = 1.0
    for position, blocks in pieces:
        steps = jax.random.uniform(jax.random.fold_in(jax.random.fold_in(stream_key, 6), position), (blocks,), jnp.float32, low / len(pieces), largest / len(pieces))
        loudness = loudness * jnp.repeat(jnp.exp(steps), shape[position] // blocks).reshape((-1,) + (1,) * (len(shape) - 1 - position))
    return loudness


def assign_block(stream_key, own, number, rows, amount, top, most, slope):
    ranking = jax.random.permutation(stream_key, amount)
    packed, common = shares(amount, rows * top, most, slope, True), shares(amount, rows * top, most, slope, False)
    places = jnp.arange(amount)

    def named(tallies, offset_by):
        used = int((tallies > 0).sum())
        fixed = max(1, used // 4)
        passed = fixed + (places - fixed + offset_by * (used - fixed)) % max(1, amount - fixed)
        return jnp.zeros((amount,), jnp.int32).at[ranking[jnp.where(places < fixed, places, passed)]].set(jnp.asarray(tallies, jnp.int32))

    tallies = jnp.where(number % 4 == 0, named(packed, number // 4), named(common, number - number // 4 - 1))
    mixed = jax.random.permutation(jax.random.fold_in(own, 3), amount)
    donor, taker = mixed[0:amount // 2 * 2:2], mixed[1:amount // 2 * 2:2]
    margin = jnp.minimum(tallies[donor] - 1, most - tallies[taker]) // 2
    margin = jnp.where((donor == ranking[0]) | (taker == ranking[0]) | (tallies[taker] == 0), 0, jnp.maximum(margin, 0))
    passed = jax.random.randint(jax.random.fold_in(own, 4), (amount // 2,), 0, 1 << 20) % (margin + 1)
    tallies = tallies.at[donor].add(-passed).at[taker].add(passed)
    members = jnp.searchsorted(jnp.cumsum(tallies), jnp.arange(rows * top), side="right").astype(jnp.int32)
    table = members.reshape(top, rows).T
    table = table[jax.random.permutation(jax.random.fold_in(own, 1), rows)]
    offset_by = jax.random.randint(jax.random.fold_in(own, 2), (rows, 1), 0, top)
    return jnp.take_along_axis(table, (jnp.arange(top)[None, :] + offset_by) % top, axis=1)


def shares(count, total, reach, slope, full):
    portions = [(1 << 20) // math.isqrt(rank ** slope) + 1 for rank in range(1, count + 1)]
    largest = reach if full else min(reach, max(-(-total // count), total * portions[0] // sum(portions)))
    least = 1 if total - largest >= count - 1 else 0
    holding, rest = [largest] + [least] * (count - 1), total - largest - least * (count - 1)
    while rest > 0:
        movable = [i for i in range(1, count) if holding[i] < largest] or [i for i in range(1, count) if holding[i] < reach]
        pool, left = sum([portions[i] for i in movable]), rest
        for i in movable:
            extra = min(reach - holding[i], max(1, left * portions[i] // pool), rest)
            holding[i] = holding[i] + extra
            rest = rest - extra
    return np.array(holding)


def scatter_about(key, extent, deviation, bound, cuts=(), kind=jnp.bfloat16):
    level = block_scale(key, extent, cuts, -0.22, 0.18) if cuts else 1.0
    entries = jax.random.normal(key, extent, jnp.float32) * deviation * level
    return jnp.minimum(jnp.maximum(entries, -bound), bound).astype(kind)


def setup_inputs(seed: int = 0) -> dict:
    key_list = jax.random.split(jax.random.key(seed), 30)
    tokens = draw_tokens(jax.random.fold_in(key_list[29], 71), 0)
    input_window = scatter_about(key_list[1], (BATCH, CONV - 1, INNER), 1.0, 6.0, ((0, 128), (2, 4)))
    write_window = scatter_about(key_list[2], (BATCH, CONV - 1, LATENT), 1.0, 6.0, ((0, 128), (2, 4)))
    read_window = scatter_about(key_list[3], (BATCH, CONV - 1, LATENT), 1.0, 6.0, ((0, 128), (2, 4)))
    ssm_state = scatter_about(key_list[4], (BATCH, HEADS, HEAD_DIM, STATE), 1.0, 6.0, ((0, 128), (1, 4)), jnp.float32)
    norm_gain = jnp.clip(1.0 + 0.18 * jax.random.normal(key_list[5], (D,), jnp.float32), 0.099609375, 1.8984375).astype(jnp.bfloat16)
    proj_gate = scatter_about(key_list[6], (D, INNER), D ** -0.5, 0.1875, ((1, 4),))
    proj_input = scatter_about(key_list[7], (D, INNER), D ** -0.5, 0.1875, ((1, 4),))
    proj_write = scatter_about(key_list[8], (D, LATENT), D ** -0.5, 0.1875, ((1, 4),))
    proj_read = scatter_about(key_list[9], (D, LATENT), D ** -0.5, 0.1875, ((1, 4),))
    proj_step = scatter_about(key_list[10], (D, HEADS), D ** -0.5, 0.1875)
    taps_input = scatter_about(key_list[11], (CONV, INNER), CONV ** -0.5, 3.0, ((1, 4),))
    taps_write = scatter_about(key_list[12], (CONV, LATENT), CONV ** -0.5, 3.0, ((1, 4),))
    taps_read = scatter_about(key_list[13], (CONV, LATENT), CONV ** -0.5, 3.0, ((1, 4),))
    step_bias = jnp.clip(jax.random.uniform(key_list[14], (HEADS,), jnp.float32, -2.5, 0.5), -2.5, 0.5)
    decay_rate = jnp.clip(jnp.exp(jax.random.uniform(key_list[15], (HEADS,), jnp.float32, math.log(0.02), math.log(2.0))), 0.02, 2.0)
    skip_gain = jnp.clip(1.0 + 0.18 * jax.random.normal(key_list[16], (HEADS,), jnp.float32), 0.1, 1.9)
    out_gain = jnp.clip(1.0 + 0.18 * jax.random.normal(key_list[17], (INNER,), jnp.float32), 0.099609375, 1.8984375).astype(jnp.bfloat16)
    proj_out = scatter_about(key_list[18], (INNER, D), INNER ** -0.5, 0.25, ((0, 4),))
    ffn_gain = jnp.clip(1.0 + 0.18 * jax.random.normal(key_list[19], (D,), jnp.float32), 0.099609375, 1.8984375).astype(jnp.bfloat16)
    expert_ids_keys = jax.random.split(jax.random.fold_in(key_list[20], 1), BATCH // SEQ_DEV)
    expert_ids_turns = jax.random.permutation(jax.random.fold_in(key_list[20], 3), BATCH // SEQ_DEV)
    expert_ids = jax.vmap(lambda own, number: assign_block(jax.random.fold_in(key_list[20], 2), own, number, SEQ_DEV, EXPERTS, TOPK, CAP, 2))(expert_ids_keys, expert_ids_turns).reshape((BATCH, TOPK))
    expert_weights = jnp.clip(jnp.exp(math.log(1.0) - 2.9957323 * jax.random.uniform(key_list[21], (BATCH, TOPK), jnp.float32) ** block_scale(key_list[21], (BATCH, TOPK), ((0, 128),), -0.2, 0.2)), 0.05, 1.0)
    expert_gate = scatter_about(key_list[22], (EXPERTS, D, EXP_FF), D ** -0.5, 0.1875, ((0, 128), (2, 4)))
    expert_up = scatter_about(key_list[23], (EXPERTS, D, EXP_FF), D ** -0.5, 0.1875, ((0, 128), (2, 4)))
    expert_down = scatter_about(key_list[24], (EXPERTS, EXP_FF, D), EXP_FF ** -0.5, 0.25, ((0, 128), (1, 4)))
    dense_gate = scatter_about(key_list[25], (D, DENSE_FF), D ** -0.5, 0.1875, ((1, 4),))
    dense_up = scatter_about(key_list[26], (D, DENSE_FF), D ** -0.5, 0.1875, ((1, 4),))
    dense_down = scatter_about(key_list[27], (D, DENSE_FF), (DENSE_FF // 8) ** -0.5, 0.5, ((1, 4),))
    branch_gate = scatter_about(key_list[28], (D,), D ** -0.5, 0.1875)
    return {"tokens": tokens, "input_window": input_window, "write_window": write_window, "read_window": read_window, "ssm_state": ssm_state, "norm_gain": norm_gain, "proj_gate": proj_gate, "proj_input": proj_input, "proj_write": proj_write, "proj_read": proj_read, "proj_step": proj_step, "taps_input": taps_input, "taps_write": taps_write, "taps_read": taps_read, "step_bias": step_bias, "decay_rate": decay_rate, "skip_gain": skip_gain, "out_gain": out_gain, "proj_out": proj_out, "ffn_gain": ffn_gain, "expert_ids": expert_ids, "expert_weights": expert_weights, "expert_gate": expert_gate, "expert_up": expert_up, "expert_down": expert_down, "dense_gate": dense_gate, "dense_up": dense_up, "dense_down": dense_down, "branch_gate": branch_gate}


EPS = 1e-06

def rms_rows(values, gain):
    widened = values.astype(jnp.float32)
    scale = lax.rsqrt(lax.optimization_barrier(jnp.mean(widened * widened, axis=-1, keepdims=True)) + EPS)
    return widened * scale * gain.astype(jnp.float32)

def short_conv(window, newest, taps):
    stacked = jnp.concatenate([window, newest[:, None, :]], axis=1)
    mixed = lax.optimization_barrier(jnp.sum(stacked.astype(jnp.float32) * taps.astype(jnp.float32)[None], axis=1))
    return (jax.nn.silu(mixed), stacked[:, 1:, :])

def round_trip(values):
    return lax.optimization_barrier(values.astype(jnp.bfloat16)).astype(jnp.float32)

def routed_outputs(normed_ffn, expert_ids, expert_gate, expert_up, expert_down):
    row_count = normed_ffn.shape[0]
    flat_ids = expert_ids.reshape(-1).astype(jnp.int32)
    order = jnp.argsort(flat_ids, stable=True).astype(jnp.int32)
    counts = lax.optimization_barrier(jnp.sum((flat_ids[:, None] == jnp.arange(EXPERTS, dtype=jnp.int32)[None, :]).astype(jnp.int32), axis=0))
    starts = (jnp.cumsum(counts) - counts).astype(jnp.int32)
    most = N_EP * CAP
    padded = jnp.concatenate([order, jnp.zeros((most,), jnp.int32)])
    slot_iota = jnp.arange(most, dtype=jnp.int32)

    def visit(totals, expert):
        picked = lax.dynamic_slice(padded, (starts[expert],), (most,))
        live = slot_iota < counts[expert]
        inputs = normed_ffn[picked // TOPK]
        gate_part = jnp.dot(inputs, expert_gate[expert], preferred_element_type=jnp.float32)
        up_part = jnp.dot(inputs, expert_up[expert], preferred_element_type=jnp.float32)
        hidden = (jax.nn.silu(gate_part) * up_part).astype(jnp.bfloat16)
        blocks = jnp.einsum('mtf,tfd->mtd', hidden.reshape(most, N_TP, FF_DEV).astype(jnp.float32), expert_down[expert].reshape(N_TP, FF_DEV, D).astype(jnp.float32))
        summed = lax.optimization_barrier(jnp.sum(round_trip(blocks), axis=1))
        result = round_trip(summed)
        return (totals.at[picked].add(jnp.where(live[:, None], result, 0.0)), None)
    start_totals = jnp.zeros((row_count * TOPK, D), jnp.float32)
    totals = lax.scan(visit, start_totals, jnp.arange(EXPERTS, dtype=jnp.int32))[0]
    return totals.reshape(row_count, TOPK, D)

def reference(tokens, input_window, write_window, read_window, ssm_state, norm_gain, proj_gate, proj_input, proj_write, proj_read, proj_step, taps_input, taps_write, taps_read, step_bias, decay_rate, skip_gain, out_gain, proj_out, ffn_gain, expert_ids, expert_weights, expert_gate, expert_up, expert_down, dense_gate, dense_up, dense_down, branch_gate):
    row_count = tokens.shape[0]
    normed = rms_rows(tokens, norm_gain).astype(jnp.bfloat16)
    gate_rows = jnp.dot(normed, proj_gate, preferred_element_type=jnp.float32).astype(jnp.bfloat16)
    input_rows = jnp.dot(normed, proj_input, preferred_element_type=jnp.float32).astype(jnp.bfloat16)
    write_rows = jnp.dot(normed, proj_write, preferred_element_type=jnp.float32).astype(jnp.bfloat16)
    read_rows = jnp.dot(normed, proj_read, preferred_element_type=jnp.float32).astype(jnp.bfloat16)
    step_raw = jnp.dot(normed, proj_step, preferred_element_type=jnp.float32)
    input_conv, new_input_window = short_conv(input_window, input_rows, taps_input)
    write_conv, new_write_window = short_conv(write_window, write_rows, taps_write)
    read_conv, new_read_window = short_conv(read_window, read_rows, taps_read)
    step_size = jax.nn.softplus(step_raw + step_bias.astype(jnp.float32))
    decay = jnp.exp(-step_size * decay_rate.astype(jnp.float32))
    heads_input = input_conv.reshape(row_count, HEADS, HEAD_DIM)
    per_group = HEADS // BC_GROUPS
    write_heads = jnp.repeat(write_conv.reshape(row_count, BC_GROUPS, STATE), per_group, axis=1)
    read_heads = jnp.repeat(read_conv.reshape(row_count, BC_GROUPS, STATE), per_group, axis=1)
    new_state = decay[:, :, None, None] * ssm_state + (step_size[:, :, None] * heads_input)[:, :, :, None] * write_heads[:, :, None, :]
    readout = jnp.einsum('bhpn,bhn->bhp', new_state, read_heads, precision=lax.Precision.HIGHEST)
    readout = readout + skip_gain.astype(jnp.float32)[None, :, None] * heads_input
    gated = readout.reshape(row_count, INNER) * jax.nn.silu(gate_rows.astype(jnp.float32))
    grouped = gated.reshape(row_count, BC_GROUPS, INNER // BC_GROUPS)
    grouped = grouped * lax.rsqrt(lax.optimization_barrier(jnp.mean(grouped * grouped, axis=-1, keepdims=True)) + EPS)
    mixer_rows = (grouped.reshape(row_count, INNER) * out_gain.astype(jnp.float32)).astype(jnp.bfloat16)
    blocks = jnp.einsum('btk,tkd->btd', mixer_rows.reshape(row_count, N_TP, INNER // N_TP).astype(jnp.float32), proj_out.reshape(N_TP, INNER // N_TP, D).astype(jnp.float32))
    mixed = lax.optimization_barrier(jnp.sum(round_trip(blocks), axis=1))
    hidden_rows = (tokens.astype(jnp.float32) + mixed).astype(jnp.bfloat16)
    normed_ffn = rms_rows(hidden_rows, ffn_gain).astype(jnp.bfloat16)
    routed = routed_outputs(normed_ffn, expert_ids, expert_gate, expert_up, expert_down)
    expert_sum = lax.optimization_barrier(jnp.sum(expert_weights.astype(jnp.float32)[:, :, None] * routed, axis=1))
    dense_gate_part = jnp.dot(normed_ffn, dense_gate, preferred_element_type=jnp.float32)
    dense_up_part = jnp.dot(normed_ffn, dense_up, preferred_element_type=jnp.float32)
    dense_hidden = (jax.nn.silu(dense_gate_part) * dense_up_part).astype(jnp.bfloat16)
    dense_sum = lax.dot_general(dense_hidden, dense_down, (((1,), (1,)), ((), ())), preferred_element_type=jnp.float32)
    branch = jax.nn.sigmoid(jnp.dot(normed_ffn, branch_gate, preferred_element_type=jnp.float32))
    new_hidden = (hidden_rows.astype(jnp.float32) + expert_sum + branch[:, None] * dense_sum).astype(jnp.bfloat16)
    return (new_hidden, new_state, new_input_window, new_write_window, new_read_window)
```

```python
import functools

import jax
import jax.numpy as jnp
from jax import lax
from jax.experimental import pallas as pl
from jax.experimental.pallas import tpu as pltpu
from jax.sharding import PartitionSpec as P

HEADS = 8
HEAD_DIM = 64
STATE = 64
EPS = 1e-06
F32 = jnp.float32
BF16 = jnp.bfloat16

HBM = pl.BlockSpec(memory_space=pltpu.HBM)
VMEM = pl.BlockSpec(memory_space=pltpu.VMEM)
SMEM = pl.BlockSpec(memory_space=pltpu.SMEM)
INTERPRET = False
LIMIT = 16 * 1024 * 1024


def call(body, outs, specs, name, scratch=(), out_spec=VMEM):
    return pl.pallas_call(
        body,
        out_shape=outs,
        in_specs=specs,
        out_specs=jax.tree.map(lambda _: out_spec, outs),
        scratch_shapes=scratch,
        compiler_params=pltpu.CompilerParams(vmem_limit_bytes=LIMIT),
        name=name,
        interpret=INTERPRET,
    )


def kept(value):
    return pltpu.with_memory_space_constraint(value, pltpu.HBM)


def sds(shape, dtype):
    return jax.ShapeDtypeStruct(shape, dtype)


def nt(a, b):
    return lax.dot_general(a, b, (((1,), (1,)), ((), ())), preferred_element_type=F32)


def nn(a, b):
    return jnp.dot(a, b, preferred_element_type=F32)


def silu(v):
    return v / (1.0 + jnp.exp(-v))


def softplus(v):
    return jnp.maximum(v, 0.0) + jnp.log1p(jnp.exp(-jnp.abs(v)))


def spread_body(tokens, out, sems):
    copies = [
        pltpu.make_async_copy(tokens, out.at[j], sems.at[j]) for j in range(out.shape[0])
    ]
    for copy in copies:
        copy.start()
    for copy in copies:
        copy.wait()


def zeros_and_ones(shape, test):
    across = lax.broadcasted_iota(jnp.int32, shape, 1)
    down = lax.broadcasted_iota(jnp.int32, shape, 0)
    return test(down, across).astype(F32).astype(BF16)


def route(rank, ids, weights, select, combine):
    tops, rows = ids.shape
    experts = combine.shape[1] // 8
    pieces = select.shape[0] // experts
    expert = lax.broadcasted_iota(jnp.int32, (experts, rows), 0)
    hits = jnp.zeros((experts, rows), F32)
    amount = jnp.zeros((experts, rows), F32)
    for k in range(tops):
        same = expert == ids[k : k + 1, :]
        hits = jnp.where(same, 1.0, hits)
        amount = jnp.where(same, weights[k : k + 1, :], amount)
    earlier = zeros_and_ones((rows, rows), lambda d, a: d < a)
    place = nn(hits.astype(BF16), earlier)
    mine = jnp.bitwise_and(rank[0], 1).astype(F32)
    chosen = jnp.where(place == mine, hits, 0.0).astype(BF16)
    down = zeros_and_ones((experts * pieces, experts), lambda d, a: d // pieces == a)
    across = zeros_and_ones((rows, rows * pieces), lambda d, a: a // pieces == d)
    wide = nn(nn(down, chosen).astype(BF16), across)
    matched = zeros_and_ones(wide.shape, lambda d, a: d % pieces == a % pieces)
    select[...] = wide.astype(BF16) * matched
    twice = zeros_and_ones((experts, experts * 2), lambda d, a: a // 2 == d)
    halves = lax.broadcasted_iota(jnp.int32, (rows, experts * 2), 1) % 2
    for s in range(2):
        part = jnp.where(place == float(s), amount, 0.0).T
        high = part.astype(BF16)
        low = (part - high.astype(F32)).astype(BF16)
        for p, piece in enumerate((high, low)):
            both = nn(piece, twice)
            for h in range(2):
                rows_at = (2 * p + h) * rows
                kept = jnp.where(halves == h, both, 0.0).astype(BF16)
                for t in (s, s + 2):
                    combine[
                        rows_at : rows_at + rows, t * 2 * experts : (t + 1) * 2 * experts
                    ] = kept


STAGED = 14


def prepare_body(*refs):
    rank, ids, weights, bias, rate, skip, gate, up, down = refs[:9]
    sources = refs[9 : 9 + STAGED]
    select, combine, lanes, packed = refs[9 + STAGED : 13 + STAGED]
    targets = refs[13 + STAGED : 13 + 2 * STAGED]
    ids_here, weights_here, bias_here, rate_here, skip_here, sems = refs[13 + 2 * STAGED :]
    width, block = gate.shape
    pairs = [
        (ids, ids_here),
        (weights, weights_here),
        (bias, bias_here),
        (rate, rate_here),
        (skip, skip_here),
    ]
    pairs += list(zip(sources, targets))
    pairs += [(gate, packed.at[0:width]), (up, packed.at[width : 2 * width])]
    for j in range(width // block):
        first = 2 * width + j * block
        pairs.append((down.at[:, j * block : (j + 1) * block], packed.at[first : first + block]))
    copies = [pltpu.make_async_copy(a, b, sems.at[k]) for k, (a, b) in enumerate(pairs)]
    for copy in copies:
        copy.start()
    for copy in copies[:5]:
        copy.wait()
    route(rank, ids_here, weights_here, select, combine)
    inner = lanes.shape[1]
    heads = inner // HEAD_DIM
    lane_head = lax.broadcasted_iota(jnp.int32, (1, inner), 1) // HEAD_DIM
    for k, table in enumerate((bias_here, rate_here, skip_here)):
        line = jnp.zeros((1, inner), F32)
        for h in range(heads):
            line = jnp.where(lane_head == h, table[rank[0] * heads + h], line)
        lanes[k : k + 1, :] = line
    for copy in copies[5:]:
        copy.wait()


def conv(window, newest, taps, out_window):
    taken = taps[...].astype(F32)
    total = newest.astype(F32) * taken[3:4]
    for k in range(3):
        total += window[k].astype(F32) * taken[k : k + 1]
    out_window[0] = window[1]
    out_window[1] = window[2]
    out_window[2] = newest
    return silu(total)


def mixer_body(
    rank,
    lanes,
    arrived,
    norm_gain,
    proj_gate,
    proj_input,
    proj_write,
    proj_read,
    proj_step,
    taps_input,
    taps_write,
    taps_read,
    input_window,
    write_window,
    read_window,
    state,
    out_gain,
    proj_out,
    partial,
    new_state,
    new_input_window,
    new_write_window,
    new_read_window,
):
    rows = arrived.shape[1]
    x = jnp.concatenate([arrived[j] for j in range(arrived.shape[0])], axis=1).astype(F32)
    scale = lax.rsqrt(jnp.mean(x * x, axis=-1, keepdims=True) + EPS)
    normed = (x * scale * norm_gain[...].astype(F32)[None, :]).astype(BF16)
    gate_rows = nn(normed, proj_gate[...]).astype(BF16)
    input_rows = nn(normed, proj_input[...]).astype(BF16)
    write_rows = nt(normed, proj_write[...]).astype(BF16)
    read_rows = nt(normed, proj_read[...]).astype(BF16)
    step_all = nt(normed, proj_step[...])
    input_conv = conv(input_window, input_rows, taps_input, new_input_window)
    write_conv = conv(write_window, write_rows, taps_write, new_write_window)
    read_conv = conv(read_window, read_rows, taps_read, new_read_window)
    inner = input_conv.shape[1]
    heads = inner // HEAD_DIM
    lane_head = lax.broadcasted_iota(jnp.int32, (rows, inner), 1) // HEAD_DIM
    column = lax.broadcasted_iota(jnp.int32, step_all.shape, 1)
    raw = jnp.zeros((rows, inner), F32)
    for h in range(heads):
        mine = column == rank[0] * heads + h
        raw = jnp.where(
            lane_head == h, jnp.sum(jnp.where(mine, step_all, 0.0), axis=1, keepdims=True), raw
        )
    step = softplus(raw + lanes[0:1, :])
    decay = jnp.exp(-step * lanes[1:2, :])
    scaled_t = (step * input_conv).T
    decay_t = decay.T
    lane = lax.broadcasted_iota(jnp.int32, (inner, rows), 1)
    readout_t = jnp.zeros((inner, rows), F32)
    for b in range(rows):
        fresh = (
            decay_t[:, b : b + 1] * state[b] + scaled_t[:, b : b + 1] * write_conv[b : b + 1, :]
        )
        new_state[b] = fresh
        seen = jnp.sum(fresh * read_conv[b : b + 1, :], axis=1, keepdims=True)
        readout_t = jnp.where(lane == b, seen, readout_t)
    readout = readout_t.T + lanes[2:3, :] * input_conv
    gated = readout * silu(gate_rows.astype(F32))
    gated = gated * lax.rsqrt(jnp.mean(gated * gated, axis=-1, keepdims=True) + EPS)
    mixer_rows = (gated * out_gain[...].astype(F32)[None, :]).astype(BF16)
    mixed = nn(mixer_rows, proj_out[...]).astype(BF16)
    for j in range(partial.shape[0]):
        partial[j] = mixed


def hidden_body(
    rank, arrived, mixed_in, ffn_gain, select, outgoing, normed_out, hidden_part, folded
):
    count, rows, quarter = arrived.shape
    x = jnp.concatenate([arrived[j] for j in range(count)], axis=1).astype(F32)
    mixed = mixed_in[0].astype(F32)
    for j in range(1, count):
        mixed += mixed_in[j].astype(F32)
    hidden = (x + mixed).astype(BF16)
    wide = hidden.astype(F32)
    scale = lax.rsqrt(jnp.mean(wide * wide, axis=-1, keepdims=True) + EPS)
    normed_wide = wide * scale * ffn_gain[...].astype(F32)[None, :]
    normed_out[...] = normed_wide.astype(BF16)
    pieces = folded.shape[0] // rows
    for j in range(pieces):
        folded[pl.ds(j, rows, stride=pieces), :] = normed_wide[:, j * 128 : (j + 1) * 128]
    outgoing[...] = nn(select[...], folded[...].astype(BF16)).astype(BF16)
    part = wide[:, 0:quarter]
    for j in range(1, count):
        part = jnp.where(rank[0] == j, wide[:, j * quarter : (j + 1) * quarter], part)
    hidden_part[...] = part.astype(BF16)


def dense_body(
    rank, normed_in, gate, up, down, branch_gate, out0, out1, out2, out3, branch, pieces
):
    normed = normed_in[...]
    hidden = (silu(nn(normed, gate[...])) * nn(normed, up[...])).astype(BF16)
    total = nt(hidden, down[...]).astype(BF16)
    quarter = out0.shape[1]
    for j in range(pieces.shape[0]):
        pieces[j] = total[:, j * quarter : (j + 1) * quarter]
    for k, out in enumerate((out0, out1, out2, out3)):
        out[...] = pieces[jnp.bitwise_and(rank[0] + k, 3)]
    level = jnp.sum(
        normed.astype(F32) * branch_gate[...].astype(F32)[None, :], axis=-1, keepdims=True
    )
    branch[...] = jnp.broadcast_to(jax.nn.sigmoid(level), branch.shape)


def expert_body(items, gate, up, down, other, out, unfolded, fold):
    width, block = gate.shape
    pieces = width // 128
    count = items.shape[0] // pieces
    unfolded[...] = items[...].astype(F32)
    x = jnp.concatenate(
        [unfolded[pl.ds(j, count, stride=pieces), :].astype(BF16) for j in range(pieces)], axis=1
    )
    act = (silu(nn(x, gate[...])) * nn(x, up[...])).astype(BF16)
    act_other = (silu(nn(x, other[0:width])) * nn(x, other[width : 2 * width])).astype(BF16)
    total = nn(act, down[...])
    for j in range(pieces):
        first = 2 * width + j * block
        piece = total[:, j * block : (j + 1) * block] + nn(act_other, other[first : first + block])
        fold[pl.ds(j // 2 * 2 * count + j % 2, count, stride=2), :] = piece
    out[...] = fold[...].astype(BF16)


def final_body(returned, combine, dense0, dense1, dense2, dense3, branch, hidden_part, out):
    total = hidden_part[...].astype(F32)
    rows = total.shape[0]
    dense = dense0[...].astype(F32)
    for piece in (dense1, dense2, dense3):
        dense += piece[...].astype(F32)
    sums = nn(combine[...], returned[...])
    sums = sums[0 : 2 * rows] + sums[2 * rows :]
    total += jnp.concatenate([sums[0:rows], sums[rows:]], axis=1)
    total += branch[:, 0:1] * dense
    out[...] = total.astype(BF16)


def local(
    tokens,
    input_window,
    write_window,
    read_window,
    ssm_state,
    norm_gain,
    proj_gate,
    proj_input,
    proj_write,
    proj_read,
    proj_step,
    taps_input,
    taps_write,
    taps_read,
    step_bias,
    decay_rate,
    skip_gain,
    out_gain,
    proj_out,
    ffn_gain,
    expert_ids,
    expert_weights,
    expert_gate,
    expert_up,
    expert_down,
    dense_gate,
    dense_up,
    dense_down,
    branch_gate,
):
    tps = lax.axis_size("tp")
    eps = lax.axis_size("ep")
    rank = lax.axis_index("tp").astype(jnp.int32).reshape(1)
    rows, quarter = tokens.shape
    width = quarter * tps
    inner = proj_gate.shape[1]
    latent = proj_write.shape[1]
    heads = ssm_state.shape[1]
    block = expert_gate.shape[2]

    pieces = width // 128

    spread = call(
        spread_body,
        sds((tps, rows, quarter), BF16),
        [HBM],
        "spread",
        [pltpu.SemaphoreType.DMA((tps,))],
        HBM,
    )(kept(tokens))
    with jax.named_scope("gather"):
        arrived = lax.all_to_all(spread, "tp", 0, 0, tiled=True)

    staged = (
        norm_gain,
        proj_gate,
        proj_input,
        proj_write.T,
        proj_read.T,
        proj_step.T,
        taps_input,
        taps_write,
        taps_read,
        input_window.transpose(1, 0, 2),
        write_window.transpose(1, 0, 2),
        read_window.transpose(1, 0, 2),
        ssm_state.reshape(rows, inner, STATE),
        out_gain,
    )
    ids, weights = expert_ids.T, expert_weights.T
    select, combine, lanes, packed, *staged = call(
        prepare_body,
        (
            sds((eps * pieces, rows * pieces), BF16),
            sds((4 * rows, 2 * tps * eps), BF16),
            sds((8, inner), F32),
            sds((3 * width, block), BF16),
        )
        + tuple(sds(v.shape, v.dtype) for v in staged),
        [SMEM] + [HBM] * (8 + STAGED),
        "prepare",
        [
            pltpu.VMEM(ids.shape, ids.dtype),
            pltpu.VMEM(weights.shape, F32),
            pltpu.SMEM(step_bias.shape, F32),
            pltpu.SMEM(step_bias.shape, F32),
            pltpu.SMEM(step_bias.shape, F32),
            pltpu.SemaphoreType.DMA((7 + pieces + STAGED,)),
        ],
    )(
        rank,
        *map(
            kept,
            (
                ids,
                weights,
                step_bias,
                decay_rate,
                skip_gain,
                expert_gate[0],
                expert_up[0],
                expert_down[0],
                *staged,
            ),
        ),
    )

    partial, new_state, new_input, new_write, new_read = call(
        mixer_body,
        (
            sds((tps, rows, width), BF16),
            sds((rows, inner, STATE), F32),
            sds((3, rows, inner), BF16),
            sds((3, rows, latent), BF16),
            sds((3, rows, latent), BF16),
        ),
        [SMEM] + [VMEM] * 17,
        "mixer",
    )(rank, lanes, arrived, *staged, proj_out)
    with jax.named_scope("mix"):
        mixed_in = lax.all_to_all(partial, "tp", 0, 0, tiled=True)
    packed, mixed_in = lax.optimization_barrier((packed, mixed_in))
    with jax.named_scope("swap"):
        other = lax.ppermute(packed, "tp", [(t, t ^ 1) for t in range(tps)])

    outgoing, normed_ffn, hidden_part = call(
        hidden_body,
        (
            sds((eps * pieces, 128), BF16),
            sds((rows, width), BF16),
            sds((rows, quarter), BF16),
        ),
        [SMEM] + [VMEM] * 4,
        "hidden",
        [pltpu.VMEM((rows * pieces, 128), F32)],
    )(rank, arrived, mixed_in, ffn_gain, select)
    items = lax.all_to_all(outgoing.reshape(eps, pieces, 128), "ep", 0, 0, tiled=True)

    dense_out = call(
        dense_body,
        (sds((rows, quarter), BF16),) * tps + (sds((rows, 128), F32),),
        [SMEM] + [VMEM] * 5,
        "dense",
        [pltpu.VMEM((tps, rows, quarter), BF16)],
    )(rank, normed_ffn, dense_gate, dense_up, dense_down, branch_gate)
    branch = dense_out[tps]
    dense_in = [dense_out[0]]
    for k in range(1, tps):
        with jax.named_scope("dense_swap"):
            turn = [(t, (t + k) % tps) for t in range(tps)]
            dense_in.append(lax.ppermute(dense_out[k], "tp", turn))

    results = call(
        expert_body,
        sds((tps * eps * 2, 128), BF16),
        [VMEM] * 5,
        "experts",
        [pltpu.VMEM((eps * pieces, 128), F32), pltpu.VMEM((tps * eps * 2, 128), F32)],
    )(items.reshape(eps * pieces, 128), expert_gate[0], expert_up[0], expert_down[0], other)
    returned = lax.all_to_all(
        results.reshape(tps * eps, 2, 128), ("tp", "ep"), 0, 0, tiled=True
    ).reshape(tps * eps * 2, 128)

    new_hidden = call(final_body, sds((rows, quarter), BF16), [VMEM] * 8, "final")(
        returned, combine, *dense_in, branch, hidden_part
    )
    return (
        new_hidden,
        new_state.reshape(rows, heads, HEAD_DIM, STATE),
        new_input.transpose(1, 0, 2),
        new_write.transpose(1, 0, 2),
        new_read.transpose(1, 0, 2),
    )


def solution(mesh):
    in_specs = (
        P("ep", "tp"),
        P("ep", None, "tp"),
        P("ep", None, "tp"),
        P("ep", None, "tp"),
        P("ep", "tp", None, None),
        P(),
        P(None, "tp"),
        P(None, "tp"),
        P(None, "tp"),
        P(None, "tp"),
        P(),
        P(None, "tp"),
        P(None, "tp"),
        P(None, "tp"),
        P(),
        P(),
        P(),
        P("tp"),
        P("tp", None),
        P(),
        P("ep", None),
        P("ep", None),
        P("ep", None, "tp"),
        P("ep", None, "tp"),
        P("ep", "tp", None),
        P(None, "tp"),
        P(None, "tp"),
        P(None, "tp"),
        P(),
    )
    out_specs = (
        P("ep", "tp"),
        P("ep", "tp", None, None),
        P("ep", None, "tp"),
        P("ep", None, "tp"),
        P("ep", None, "tp"),
    )
    return jax.shard_map(local, mesh=mesh, in_specs=in_specs, out_specs=out_specs, check_vma=False)
```

```python
import jax
import jax.numpy as jnp
from jax import lax
from jax.experimental import pallas as pl
from jax.experimental.pallas import tpu as pltpu
from jax.sharding import PartitionSpec as P


HEADS = 8
HEAD_DIM = 64
STATE = 64
EPS = 1e-06
F32 = jnp.float32
BF16 = jnp.bfloat16

HBM = pl.BlockSpec(memory_space=pltpu.HBM)
VMEM = pl.BlockSpec(memory_space=pltpu.VMEM)
SMEM = pl.BlockSpec(memory_space=pltpu.SMEM)
INTERPRET = False
LIMIT = 16 * 1024 * 1024


def call(body, outs, specs, scratch=(), out_spec=VMEM):
    return pl.pallas_call(
        body,
        out_shape=outs,
        in_specs=specs,
        out_specs=out_spec
        if isinstance(out_spec, tuple)
        else jax.tree.map(lambda _: out_spec, outs),
        scratch_shapes=scratch,
        compiler_params=pltpu.CompilerParams(vmem_limit_bytes=LIMIT),
        interpret=INTERPRET,
    )


def kept(value):
    return pltpu.with_memory_space_constraint(value, pltpu.HBM)


def sds(shape, dtype):
    return jax.ShapeDtypeStruct(shape, dtype)


def nt(a, b):
    return lax.dot_general(a, b, (((1,), (1,)), ((), ())), preferred_element_type=F32)


def nn(a, b):
    return jnp.dot(a, b, preferred_element_type=F32)


def silu(v):
    return v / (1.0 + jnp.exp(-v))


def softplus(v):
    return jnp.maximum(v, 0.0) + jnp.log1p(jnp.exp(-jnp.abs(v)))


def spread_body(tokens, out, here, sems):
    first = pltpu.make_async_copy(tokens, here, sems.at[out.shape[0]])
    first.start()
    first.wait()
    copies = [pltpu.make_async_copy(here, out.at[j], sems.at[j]) for j in range(out.shape[0])]
    for copy in copies:
        copy.start()
    for copy in copies:
        copy.wait()


def zeros_and_ones(shape, test):
    across = lax.broadcasted_iota(jnp.int32, shape, 1)
    down = lax.broadcasted_iota(jnp.int32, shape, 0)
    return test(down, across).astype(F32).astype(BF16)


def route(rank, ids, weights, select, combine):
    tops, rows = ids.shape
    experts = combine.shape[1] // 8
    pieces = select.shape[0] // experts
    expert = lax.broadcasted_iota(jnp.int32, (experts, rows), 0)
    hits = jnp.zeros((experts, rows), F32)
    amount = jnp.zeros((experts, rows), F32)
    for k in range(tops):
        same = expert == ids[k : k + 1, :]
        hits = jnp.where(same, 1.0, hits)
        amount = jnp.where(same, weights[k : k + 1, :], amount)
    earlier = zeros_and_ones((rows, rows), lambda d, a: d < a)
    place = nn(hits.astype(BF16), earlier)
    mine = jnp.bitwise_and(rank[0], 1).astype(F32)
    chosen = jnp.where(place == mine, hits, 0.0).astype(BF16)
    down = zeros_and_ones((experts * pieces, experts), lambda d, a: d // pieces == a)
    across = zeros_and_ones((rows, rows * pieces), lambda d, a: a // pieces == d)
    wide = nn(nn(down, chosen).astype(BF16), across)
    matched = zeros_and_ones(wide.shape, lambda d, a: d % pieces == a % pieces)
    select[...] = wide.astype(BF16) * matched
    twice = zeros_and_ones((experts, experts * 2), lambda d, a: a // 2 == d)
    halves = lax.broadcasted_iota(jnp.int32, (rows, experts * 2), 1) % 2
    for s in range(2):
        part = jnp.where(place == float(s), amount, 0.0).T
        high = part.astype(BF16)
        low = (part - high.astype(F32)).astype(BF16)
        for p, piece in enumerate((high, low)):
            both = nn(piece, twice)
            for h in range(2):
                rows_at = (2 * p + h) * rows
                kept = jnp.where(halves == h, both, 0.0).astype(BF16)
                for t in (s, s + 2):
                    combine[
                        rows_at : rows_at + rows, t * 2 * experts : (t + 1) * 2 * experts
                    ] = kept


STAGED = 9


def prepare_body(*refs):
    rank, ids, weights, bias, rate, skip, gate, up, down = refs[:9]
    proj_gate, proj_input, proj_write, proj_read, proj_step = refs[9:14]
    sources = refs[14 : 14 + STAGED]
    select, combine, lanes, packed, across, along = refs[14 + STAGED : 20 + STAGED]
    targets = refs[20 + STAGED : 20 + 2 * STAGED]
    ids_here, weights_here, bias_here, rate_here, skip_here, sems = refs[20 + 2 * STAGED :]
    width, block = gate.shape
    inner = proj_gate.shape[1]
    latent = proj_write.shape[0]
    pairs = [
        (ids, ids_here),
        (weights, weights_here),
        (bias, bias_here),
        (rate, rate_here),
        (skip, skip_here),
    ]
    pairs += [
        (proj_gate, across.at[:, 0:inner]),
        (proj_input, across.at[:, inner : 2 * inner]),
        (proj_write, along.at[0:latent]),
        (proj_read, along.at[latent : 2 * latent]),
        (proj_step, along.at[2 * latent : 2 * latent + HEADS]),
    ]
    pairs += list(zip(sources, targets))
    pairs += [(gate, packed.at[0:width]), (up, packed.at[width : 2 * width])]
    for j in range(width // block):
        first = 2 * width + j * block
        pairs.append((down.at[:, j * block : (j + 1) * block], packed.at[first : first + block]))
    copies = [pltpu.make_async_copy(a, b, sems.at[k]) for k, (a, b) in enumerate(pairs)]
    for copy in copies:
        copy.start()
    for copy in copies[:5]:
        copy.wait()
    route(rank, ids_here, weights_here, select, combine)
    heads = inner // HEAD_DIM
    lane_head = lax.broadcasted_iota(jnp.int32, (1, inner), 1) // HEAD_DIM
    for k, table in enumerate((bias_here, rate_here, skip_here)):
        line = jnp.zeros((1, inner), F32)
        for h in range(heads):
            line = jnp.where(lane_head == h, table[rank[0] * heads + h], line)
        lanes[k : k + 1, :] = line
    for copy in copies[5:]:
        copy.wait()


def conv(window, newest, taps, out_window):
    taken = taps[...].astype(F32)
    total = newest.astype(F32) * taken[3:4]
    for k in range(3):
        total += window[k].astype(F32) * taken[k : k + 1]
    out_window[0] = window[1]
    out_window[1] = window[2]
    out_window[2] = newest
    return silu(total)


def mixer_body(
    rank,
    lanes,
    arrived,
    across,
    along,
    norm_gain,
    taps_input,
    taps_write,
    taps_read,
    input_window,
    write_window,
    read_window,
    state,
    out_gain,
    proj_out,
    partial,
    new_state,
    new_input_window,
    new_write_window,
    new_read_window,
):
    rows = arrived.shape[1]
    x = jnp.concatenate([arrived[j] for j in range(arrived.shape[0])], axis=1).astype(F32)
    scale = lax.rsqrt(jnp.mean(x * x, axis=-1, keepdims=True) + EPS)
    normed = (x * scale * norm_gain[...].astype(F32)[None, :]).astype(BF16)
    inner = input_window.shape[2]
    latent = write_window.shape[2]
    first = nn(normed, across[...])
    second = nt(normed, along[...])
    gate_rows = first[:, 0:inner].astype(BF16)
    input_rows = first[:, inner : 2 * inner].astype(BF16)
    write_rows = second[:, 0:latent].astype(BF16)
    read_rows = second[:, latent : 2 * latent].astype(BF16)
    step_all = second[:, 2 * latent : 2 * latent + HEADS]
    input_conv = conv(input_window, input_rows, taps_input, new_input_window)
    write_conv = conv(write_window, write_rows, taps_write, new_write_window)
    read_conv = conv(read_window, read_rows, taps_read, new_read_window)
    heads = inner // HEAD_DIM
    lane_head = lax.broadcasted_iota(jnp.int32, (rows, inner), 1) // HEAD_DIM
    column = lax.broadcasted_iota(jnp.int32, step_all.shape, 1)
    raw = jnp.zeros((rows, inner), F32)
    for h in range(heads):
        mine = column == rank[0] * heads + h
        raw = jnp.where(
            lane_head == h, jnp.sum(jnp.where(mine, step_all, 0.0), axis=1, keepdims=True), raw
        )
    step = softplus(raw + lanes[0:1, :])
    decay = jnp.exp(-step * lanes[1:2, :])
    scaled_t = (step * input_conv).T
    decay_t = decay.T
    lane = lax.broadcasted_iota(jnp.int32, (inner, rows), 1)
    readout_t = jnp.zeros((inner, rows), F32)
    for b in range(rows):
        fresh = (
            decay_t[:, b : b + 1] * state[b] + scaled_t[:, b : b + 1] * write_conv[b : b + 1, :]
        )
        new_state[b] = fresh
        seen = jnp.sum(fresh * read_conv[b : b + 1, :], axis=1, keepdims=True)
        readout_t = jnp.where(lane == b, seen, readout_t)
    readout = readout_t.T + lanes[2:3, :] * input_conv
    gated = readout * silu(gate_rows.astype(F32))
    gated = gated * lax.rsqrt(jnp.mean(gated * gated, axis=-1, keepdims=True) + EPS)
    mixer_rows = (gated * out_gain[...].astype(F32)[None, :]).astype(BF16)
    mixed = nn(mixer_rows, proj_out[...]).astype(BF16)
    for j in range(partial.shape[0]):
        partial[j] = mixed


def hidden_body(
    rank, arrived, mixed_in, ffn_gain, select, outgoing, normed_out, hidden_part, folded
):
    count, rows, quarter = arrived.shape
    x = jnp.concatenate([arrived[j] for j in range(count)], axis=1).astype(F32)
    mixed = mixed_in[0].astype(F32)
    for j in range(1, count):
        mixed += mixed_in[j].astype(F32)
    hidden = (x + mixed).astype(BF16)
    wide = hidden.astype(F32)
    scale = lax.rsqrt(jnp.mean(wide * wide, axis=-1, keepdims=True) + EPS)
    normed_wide = wide * scale * ffn_gain[...].astype(F32)[None, :]
    normed_out[...] = normed_wide.astype(BF16)
    pieces = folded.shape[0] // rows
    for j in range(pieces):
        folded[pl.ds(j, rows, stride=pieces), :] = normed_wide[:, j * 128 : (j + 1) * 128]
    outgoing[...] = nn(select[...], folded[...].astype(BF16)).astype(BF16)
    part = wide[:, 0:quarter]
    for j in range(1, count):
        part = jnp.where(rank[0] == j, wide[:, j * quarter : (j + 1) * quarter], part)
    hidden_part[...] = part.astype(BF16)


def dense_body(rank, normed_in, gate, up, down, branch_gate, give, keep, branch):
    normed = normed_in[...]
    hidden = (silu(nn(normed, gate[...])) * nn(normed, up[...])).astype(BF16)
    total = nt(hidden, down[...]).astype(BF16)
    half = give.shape[1]
    upper = rank[0] > 1
    give[...] = jnp.where(upper, total[:, 0:half], total[:, half:])
    keep[...] = jnp.where(upper, total[:, half:], total[:, 0:half])
    level = jnp.sum(
        normed.astype(F32) * branch_gate[...].astype(F32)[None, :], axis=-1, keepdims=True
    )
    branch[...] = jnp.broadcast_to(jax.nn.sigmoid(level), branch.shape)


def halve_body(rank, keep, got, give, left):
    total = keep[...].astype(F32) + got[...].astype(F32)
    quarter = give.shape[1]
    odd = jnp.bitwise_and(rank[0], 1) > 0
    give[...] = jnp.where(odd, total[:, 0:quarter], total[:, quarter:]).astype(BF16)
    left[...] = jnp.where(odd, total[:, quarter:], total[:, 0:quarter])


def expert_body(items, gate, up, down, other, out, unfolded, fold):
    width, block = gate.shape
    pieces = width // 128
    count = items.shape[0] // pieces
    unfolded[...] = items[...].astype(F32)
    x = jnp.concatenate(
        [unfolded[pl.ds(j, count, stride=pieces), :].astype(BF16) for j in range(pieces)], axis=1
    )
    act = (silu(nn(x, gate[...])) * nn(x, up[...])).astype(BF16)
    act_other = (silu(nn(x, other[0:width])) * nn(x, other[width : 2 * width])).astype(BF16)
    total = nn(act, down[...])
    for j in range(pieces):
        first = 2 * width + j * block
        piece = total[:, j * block : (j + 1) * block] + nn(act_other, other[first : first + block])
        fold[pl.ds(j // 2 * 2 * count + j % 2, count, stride=2), :] = piece
    out[...] = fold[...].astype(BF16)


def final_body(returned, combine, left, got, branch, hidden_part, out):
    total = hidden_part[...].astype(F32)
    rows = total.shape[0]
    dense = left[...] + got[...].astype(F32)
    sums = nn(combine[...], returned[...])
    sums = sums[0 : 2 * rows] + sums[2 * rows :]
    total += jnp.concatenate([sums[0:rows], sums[rows:]], axis=1)
    total += branch[:, 0:1] * dense
    out[...] = total.astype(BF16)


def local(
    tokens,
    input_window,
    write_window,
    read_window,
    ssm_state,
    norm_gain,
    proj_gate,
    proj_input,
    proj_write,
    proj_read,
    proj_step,
    taps_input,
    taps_write,
    taps_read,
    step_bias,
    decay_rate,
    skip_gain,
    out_gain,
    proj_out,
    ffn_gain,
    expert_ids,
    expert_weights,
    expert_gate,
    expert_up,
    expert_down,
    dense_gate,
    dense_up,
    dense_down,
    branch_gate,
):
    tps = lax.axis_size("tp")
    eps = lax.axis_size("ep")
    rank = lax.axis_index("tp").astype(jnp.int32).reshape(1)
    rows, quarter = tokens.shape
    width = quarter * tps
    inner = proj_gate.shape[1]
    latent = proj_write.shape[1]
    heads = ssm_state.shape[1]
    block = expert_gate.shape[2]

    pieces = width // 128

    spread = call(
        spread_body,
        sds((tps, rows, quarter), BF16),
        [HBM],
        [pltpu.VMEM((rows, quarter), BF16), pltpu.SemaphoreType.DMA((tps + 1,))],
        HBM,
    )(kept(tokens))
    arrived = lax.all_to_all(spread, "tp", 0, 0, tiled=True)

    projections = (proj_gate, proj_input, proj_write.T, proj_read.T, proj_step.T)
    staged = (
        norm_gain,
        taps_input,
        taps_write,
        taps_read,
        input_window.transpose(1, 0, 2),
        write_window.transpose(1, 0, 2),
        read_window.transpose(1, 0, 2),
        ssm_state.reshape(rows, inner, STATE),
        out_gain,
    )
    ids, weights = expert_ids.T, expert_weights.T
    select, combine, *staged = call(
        prepare_body,
        (
            pltpu.VMEM((eps * pieces, rows * pieces), BF16),
            pltpu.HBM((4 * rows, 2 * tps * eps), BF16),
            pltpu.VMEM((8, inner), F32),
            pltpu.HBM((3 * width, block), BF16),
            pltpu.VMEM((width, 2 * inner), BF16),
            pltpu.VMEM((2 * latent + HEADS, width), BF16),
        )
        + tuple(pltpu.VMEM(v.shape, v.dtype) for v in staged),
        [SMEM] + [HBM] * (13 + STAGED),
        [
            pltpu.VMEM(ids.shape, ids.dtype),
            pltpu.VMEM(weights.shape, F32),
            pltpu.SMEM(step_bias.shape, F32),
            pltpu.SMEM(step_bias.shape, F32),
            pltpu.SMEM(step_bias.shape, F32),
            pltpu.SemaphoreType.DMA((12 + pieces + STAGED,)),
        ],
        (VMEM, VMEM, VMEM, HBM) + (VMEM,) * (2 + STAGED),
    )(
        rank,
        *map(
            kept,
            (
                ids,
                weights,
                step_bias,
                decay_rate,
                skip_gain,
                expert_gate[0],
                expert_up[0],
                expert_down[0],
                *projections,
                *staged,
            ),
        ),
    )

    lanes, packed, *staged = staged
    partial, new_state, new_input, new_write, new_read = call(
        mixer_body,
        (
            pltpu.HBM((tps, rows, width), BF16),
            pltpu.VMEM((rows, inner, STATE), F32),
            pltpu.VMEM((3, rows, inner), BF16),
            pltpu.VMEM((3, rows, latent), BF16),
            pltpu.VMEM((3, rows, latent), BF16),
        ),
        [SMEM] + [VMEM] * 14,
    )(rank, lanes, arrived, *staged, proj_out)
    mixed_in = lax.all_to_all(partial, "tp", 0, 0, tiled=True)
    packed, _ = lax.optimization_barrier((packed, partial))
    other = lax.ppermute(packed, "tp", [(t, t ^ 1) for t in range(tps)])

    outgoing, normed_ffn, hidden_part = call(
        hidden_body,
        (
            sds((eps * pieces, 128), BF16),
            sds((rows, width), BF16),
            sds((rows, quarter), BF16),
        ),
        [SMEM] + [VMEM] * 4,
        [pltpu.VMEM((rows * pieces, 128), F32)],
    )(rank, arrived, mixed_in, ffn_gain, select)
    items = lax.all_to_all(outgoing.reshape(eps, pieces, 128), "ep", 0, 0, tiled=True)

    give, keep, branch = call(
        dense_body,
        (sds((rows, width // 2), BF16), sds((rows, width // 2), BF16), sds((rows, 128), F32)),
        [SMEM] + [VMEM] * 5,
    )(rank, normed_ffn, dense_gate, dense_up, dense_down, branch_gate)
    got = lax.ppermute(give, "tp", [(t, t ^ 2) for t in range(tps)])
    give, left = call(
        halve_body, (sds((rows, quarter), BF16), sds((rows, quarter), F32)), [SMEM] + [VMEM] * 2
    )(rank, keep, got)
    got = lax.ppermute(give, "tp", [(t, t ^ 1) for t in range(tps)])

    results = call(
        expert_body,
        sds((tps * eps * 2, 128), BF16),
        [VMEM] * 5,
        [pltpu.VMEM((eps * pieces, 128), F32), pltpu.VMEM((tps * eps * 2, 128), F32)],
    )(items.reshape(eps * pieces, 128), expert_gate[0], expert_up[0], expert_down[0], other)
    returned = lax.all_to_all(
        results.reshape(tps * eps, 2, 128), ("tp", "ep"), 0, 0, tiled=True
    ).reshape(tps * eps * 2, 128)

    new_hidden = call(final_body, sds((rows, quarter), BF16), [VMEM] * 6)(
        returned, combine, left, got, branch, hidden_part
    )
    return (
        new_hidden,
        new_state.reshape(rows, heads, HEAD_DIM, STATE),
        new_input.transpose(1, 0, 2),
        new_write.transpose(1, 0, 2),
        new_read.transpose(1, 0, 2),
    )


def solution(mesh):
    in_specs = (
        P("ep", "tp"),
        P("ep", None, "tp"),
        P("ep", None, "tp"),
        P("ep", None, "tp"),
        P("ep", "tp", None, None),
        P(),
        P(None, "tp"),
        P(None, "tp"),
        P(None, "tp"),
        P(None, "tp"),
        P(),
        P(None, "tp"),
        P(None, "tp"),
        P(None, "tp"),
        P(),
        P(),
        P(),
        P("tp"),
        P("tp", None),
        P(),
        P("ep", None),
        P("ep", None),
        P("ep", None, "tp"),
        P("ep", None, "tp"),
        P("ep", "tp", None),
        P(None, "tp"),
        P(None, "tp"),
        P(None, "tp"),
        P(),
    )
    out_specs = (
        P("ep", "tp"),
        P("ep", "tp", None, None),
        P("ep", None, "tp"),
        P("ep", None, "tp"),
        P("ep", None, "tp"),
    )
    return jax.shard_map(local, mesh=mesh, in_specs=in_specs, out_specs=out_specs, check_vma=False)
```

```python
import jax
import jax.numpy as jnp
from jax import lax
from jax.experimental import pallas as pl
from jax.experimental.pallas import tpu as pltpu
from jax.sharding import PartitionSpec as P


HEADS = 8
HEAD_DIM = 64
STATE = 64
EPS = 1e-06
F32 = jnp.float32
BF16 = jnp.bfloat16

HBM = pl.BlockSpec(memory_space=pltpu.HBM)
VMEM = pl.BlockSpec(memory_space=pltpu.VMEM)
SMEM = pl.BlockSpec(memory_space=pltpu.SMEM)
INTERPRET = False
LIMIT = 16 * 1024 * 1024


def call(body, outs, specs, scratch=(), out_spec=VMEM):
    return pl.pallas_call(
        body,
        out_shape=outs,
        in_specs=specs,
        out_specs=out_spec
        if isinstance(out_spec, tuple)
        else jax.tree.map(lambda _: out_spec, outs),
        scratch_shapes=scratch,
        compiler_params=pltpu.CompilerParams(vmem_limit_bytes=LIMIT),
        interpret=INTERPRET,
    )


def kept(value):
    return pltpu.with_memory_space_constraint(value, pltpu.HBM)


def sds(shape, dtype):
    return jax.ShapeDtypeStruct(shape, dtype)


def nt(a, b):
    return lax.dot_general(a, b, (((1,), (1,)), ((), ())), preferred_element_type=F32)


def nn(a, b):
    return jnp.dot(a, b, preferred_element_type=F32)


def silu(v):
    return v / (1.0 + jnp.exp(-v))


def softplus(v):
    return jnp.maximum(v, 0.0) + jnp.log1p(jnp.exp(-jnp.abs(v)))


def spread_body(tokens, out, here, sems):
    first = pltpu.make_async_copy(tokens, here, sems.at[out.shape[0]])
    first.start()
    first.wait()
    copies = [pltpu.make_async_copy(here, out.at[j], sems.at[j]) for j in range(out.shape[0])]
    for copy in copies:
        copy.start()
    for copy in copies:
        copy.wait()


def zeros_and_ones(shape, test):
    across = lax.broadcasted_iota(jnp.int32, shape, 1)
    down = lax.broadcasted_iota(jnp.int32, shape, 0)
    return test(down, across).astype(F32).astype(BF16)


def route_body(rank, ids_there, weights_there, select, combine, ids, weights, sems):
    copies = [
        pltpu.make_async_copy(ids_there, ids, sems.at[0]),
        pltpu.make_async_copy(weights_there, weights, sems.at[1]),
    ]
    for copy in copies:
        copy.start()
    for copy in copies:
        copy.wait()
    tops, rows = ids.shape
    experts = combine.shape[1] // 8
    pieces = select.shape[0] // experts
    expert = lax.broadcasted_iota(jnp.int32, (experts, rows), 0)
    hits = jnp.zeros((experts, rows), F32)
    amount = jnp.zeros((experts, rows), F32)
    for k in range(tops):
        same = expert == ids[k : k + 1, :]
        hits = jnp.where(same, 1.0, hits)
        amount = jnp.where(same, weights[k : k + 1, :], amount)
    earlier = zeros_and_ones((rows, rows), lambda d, a: d < a)
    place = nn(hits.astype(BF16), earlier)
    mine = jnp.bitwise_and(rank[0], 1).astype(F32)
    chosen = jnp.where(place == mine, hits, 0.0).astype(BF16)
    down = zeros_and_ones((experts * pieces, experts), lambda d, a: d // pieces == a)
    across = zeros_and_ones((rows, rows * pieces), lambda d, a: a // pieces == d)
    wide = nn(nn(down, chosen).astype(BF16), across)
    matched = zeros_and_ones(wide.shape, lambda d, a: d % pieces == a % pieces)
    select[...] = wide.astype(BF16) * matched
    twice = zeros_and_ones((experts, experts * 2), lambda d, a: a // 2 == d)
    halves = lax.broadcasted_iota(jnp.int32, (rows, experts * 2), 1) % 2
    for s in range(2):
        part = jnp.where(place == float(s), amount, 0.0).T
        high = part.astype(BF16)
        low = (part - high.astype(F32)).astype(BF16)
        for p, piece in enumerate((high, low)):
            both = nn(piece, twice)
            for h in range(2):
                rows_at = (2 * p + h) * rows
                kept = jnp.where(halves == h, both, 0.0).astype(BF16)
                for t in (s, s + 2):
                    combine[
                        rows_at : rows_at + rows, t * 2 * experts : (t + 1) * 2 * experts
                    ] = kept


STAGED = 9


def prepare_body(*refs):
    rank, bias, rate, skip, gate, up, down = refs[:7]
    proj_gate, proj_input, proj_write, proj_read, proj_step = refs[7:12]
    sources = refs[12 : 12 + STAGED]
    lanes, packed, across, along = refs[12 + STAGED : 16 + STAGED]
    targets = refs[16 + STAGED : 16 + 2 * STAGED]
    bias_here, rate_here, skip_here, built, sems = refs[16 + 2 * STAGED :]
    width, block = gate.shape
    inner = proj_gate.shape[1]
    latent = proj_write.shape[0]
    pairs = [
        (bias, bias_here),
        (rate, rate_here),
        (skip, skip_here),
    ]
    pairs += [(gate, built.at[0:width]), (up, built.at[width : 2 * width])]
    for j in range(width // block):
        first = 2 * width + j * block
        pairs.append((down.at[:, j * block : (j + 1) * block], built.at[first : first + block]))
    building = len(pairs)
    pairs += [
        (proj_gate, across.at[:, 0:inner]),
        (proj_input, across.at[:, inner : 2 * inner]),
        (proj_write, along.at[0:latent]),
        (proj_read, along.at[latent : 2 * latent]),
        (proj_step, along.at[2 * latent : 2 * latent + HEADS]),
    ]
    pairs += list(zip(sources, targets))
    copies = [pltpu.make_async_copy(a, b, sems.at[k]) for k, (a, b) in enumerate(pairs)]
    out_copy = pltpu.make_async_copy(built, packed, sems.at[len(pairs)])
    for copy in copies:
        copy.start()
    for copy in copies[:building]:
        copy.wait()
    out_copy.start()
    heads = inner // HEAD_DIM
    lane_head = lax.broadcasted_iota(jnp.int32, (1, inner), 1) // HEAD_DIM
    for k, table in enumerate((bias_here, rate_here, skip_here)):
        line = jnp.zeros((1, inner), F32)
        for h in range(heads):
            line = jnp.where(lane_head == h, table[rank[0] * heads + h], line)
        lanes[k : k + 1, :] = line
    for copy in copies[building:]:
        copy.wait()
    out_copy.wait()


def conv(window, newest, taps, out_window):
    taken = taps[...].astype(F32)
    total = newest.astype(F32) * taken[3:4]
    for k in range(3):
        total += window[k].astype(F32) * taken[k : k + 1]
    out_window[0] = window[1]
    out_window[1] = window[2]
    out_window[2] = newest
    return silu(total)


def mixer_body(
    rank,
    lanes,
    arrived,
    across,
    along,
    norm_gain,
    taps_input,
    taps_write,
    taps_read,
    input_window,
    write_window,
    read_window,
    state,
    out_gain,
    proj_out,
    partial,
    new_state,
    new_input_window,
    new_write_window,
    new_read_window,
):
    rows = arrived.shape[1]
    x = jnp.concatenate([arrived[j] for j in range(arrived.shape[0])], axis=1).astype(F32)
    scale = lax.rsqrt(jnp.mean(x * x, axis=-1, keepdims=True) + EPS)
    normed = (x * scale * norm_gain[...].astype(F32)[None, :]).astype(BF16)
    inner = input_window.shape[2]
    latent = write_window.shape[2]
    first = nn(normed, across[...])
    second = nt(normed, along[...])
    gate_rows = first[:, 0:inner].astype(BF16)
    input_rows = first[:, inner : 2 * inner].astype(BF16)
    write_rows = second[:, 0:latent].astype(BF16)
    read_rows = second[:, latent : 2 * latent].astype(BF16)
    step_all = second[:, 2 * latent : 2 * latent + HEADS]
    input_conv = conv(input_window, input_rows, taps_input, new_input_window)
    write_conv = conv(write_window, write_rows, taps_write, new_write_window)
    read_conv = conv(read_window, read_rows, taps_read, new_read_window)
    heads = inner // HEAD_DIM
    lane_head = lax.broadcasted_iota(jnp.int32, (rows, inner), 1) // HEAD_DIM
    column = lax.broadcasted_iota(jnp.int32, step_all.shape, 1)
    raw = jnp.zeros((rows, inner), F32)
    for h in range(heads):
        mine = column == rank[0] * heads + h
        raw = jnp.where(
            lane_head == h, jnp.sum(jnp.where(mine, step_all, 0.0), axis=1, keepdims=True), raw
        )
    step = softplus(raw + lanes[0:1, :])
    decay = jnp.exp(-step * lanes[1:2, :])
    scaled_t = (step * input_conv).T
    decay_t = decay.T
    lane = lax.broadcasted_iota(jnp.int32, (inner, rows), 1)
    readout_t = jnp.zeros((inner, rows), F32)
    for b in range(rows):
        fresh = (
            decay_t[:, b : b + 1] * state[b] + scaled_t[:, b : b + 1] * write_conv[b : b + 1, :]
        )
        new_state[b] = fresh
        seen = jnp.sum(fresh * read_conv[b : b + 1, :], axis=1, keepdims=True)
        readout_t = jnp.where(lane == b, seen, readout_t)
    readout = readout_t.T + lanes[2:3, :] * input_conv
    gated = readout * silu(gate_rows.astype(F32))
    gated = gated * lax.rsqrt(jnp.mean(gated * gated, axis=-1, keepdims=True) + EPS)
    mixer_rows = (gated * out_gain[...].astype(F32)[None, :]).astype(BF16)
    mixed = nn(mixer_rows, proj_out[...]).astype(BF16)
    for j in range(partial.shape[0]):
        partial[j] = mixed


def hidden_body(
    rank, arrived, mixed_in, ffn_gain, select, outgoing, normed_out, hidden_part, folded
):
    count, rows, quarter = arrived.shape
    x = jnp.concatenate([arrived[j] for j in range(count)], axis=1).astype(F32)
    mixed = mixed_in[0].astype(F32)
    for j in range(1, count):
        mixed += mixed_in[j].astype(F32)
    hidden = (x + mixed).astype(BF16)
    wide = hidden.astype(F32)
    scale = lax.rsqrt(jnp.mean(wide * wide, axis=-1, keepdims=True) + EPS)
    normed_wide = wide * scale * ffn_gain[...].astype(F32)[None, :]
    normed_out[...] = normed_wide.astype(BF16)
    pieces = folded.shape[0] // rows
    for j in range(pieces):
        folded[pl.ds(j, rows, stride=pieces), :] = normed_wide[:, j * 128 : (j + 1) * 128]
    outgoing[...] = nn(select[...], folded[...].astype(BF16)).astype(BF16)
    part = wide[:, 0:quarter]
    for j in range(1, count):
        part = jnp.where(rank[0] == j, wide[:, j * quarter : (j + 1) * quarter], part)
    hidden_part[...] = part.astype(BF16)


def dense_body(rank, normed_in, gate, up, down, branch_gate, give, keep, branch):
    normed = normed_in[...]
    hidden = (silu(nn(normed, gate[...])) * nn(normed, up[...])).astype(BF16)
    total = nt(hidden, down[...]).astype(BF16)
    half = give.shape[1]
    upper = rank[0] > 1
    give[...] = jnp.where(upper, total[:, 0:half], total[:, half:])
    keep[...] = jnp.where(upper, total[:, half:], total[:, 0:half])
    level = jnp.sum(
        normed.astype(F32) * branch_gate[...].astype(F32)[None, :], axis=-1, keepdims=True
    )
    branch[...] = jnp.broadcast_to(jax.nn.sigmoid(level), branch.shape)


def halve_body(rank, keep, got, give, left):
    total = keep[...].astype(F32) + got[...].astype(F32)
    quarter = give.shape[1]
    odd = jnp.bitwise_and(rank[0], 1) > 0
    give[...] = jnp.where(odd, total[:, 0:quarter], total[:, quarter:]).astype(BF16)
    left[...] = jnp.where(odd, total[:, quarter:], total[:, 0:quarter])


def expert_body(items, gate, up, down, other, out, unfolded, fold):
    width, block = gate.shape
    pieces = width // 128
    count = items.shape[0] // pieces
    unfolded[...] = items[...].astype(F32)
    x = jnp.concatenate(
        [unfolded[pl.ds(j, count, stride=pieces), :].astype(BF16) for j in range(pieces)], axis=1
    )
    act = (silu(nn(x, gate[...])) * nn(x, up[...])).astype(BF16)
    act_other = (silu(nn(x, other[0:width])) * nn(x, other[width : 2 * width])).astype(BF16)
    total = nn(act, down[...])
    for j in range(pieces):
        first = 2 * width + j * block
        piece = total[:, j * block : (j + 1) * block] + nn(act_other, other[first : first + block])
        fold[pl.ds(j // 2 * 2 * count + j % 2, count, stride=2), :] = piece
    out[...] = fold[...].astype(BF16)


def final_body(returned, combine, left, got, branch, hidden_part, out):
    total = hidden_part[...].astype(F32)
    rows = total.shape[0]
    dense = left[...] + got[...].astype(F32)
    sums = nn(combine[...], returned[...])
    sums = sums[0 : 2 * rows] + sums[2 * rows :]
    total += jnp.concatenate([sums[0:rows], sums[rows:]], axis=1)
    total += branch[:, 0:1] * dense
    out[...] = total.astype(BF16)


def local(
    tokens,
    input_window,
    write_window,
    read_window,
    ssm_state,
    norm_gain,
    proj_gate,
    proj_input,
    proj_write,
    proj_read,
    proj_step,
    taps_input,
    taps_write,
    taps_read,
    step_bias,
    decay_rate,
    skip_gain,
    out_gain,
    proj_out,
    ffn_gain,
    expert_ids,
    expert_weights,
    expert_gate,
    expert_up,
    expert_down,
    dense_gate,
    dense_up,
    dense_down,
    branch_gate,
):
    tps = lax.axis_size("tp")
    eps = lax.axis_size("ep")
    rank = lax.axis_index("tp").astype(jnp.int32).reshape(1)
    rows, quarter = tokens.shape
    width = quarter * tps
    inner = proj_gate.shape[1]
    latent = proj_write.shape[1]
    heads = ssm_state.shape[1]
    block = expert_gate.shape[2]

    pieces = width // 128

    spread = call(
        spread_body,
        sds((tps, rows, quarter), BF16),
        [HBM],
        [pltpu.VMEM((rows, quarter), BF16), pltpu.SemaphoreType.DMA((tps + 1,))],
        HBM,
    )(kept(tokens))
    arrived = lax.all_to_all(spread, "tp", 0, 0, tiled=True)

    projections = (proj_gate, proj_input, proj_write.T, proj_read.T, proj_step.T)
    staged = (
        norm_gain,
        taps_input,
        taps_write,
        taps_read,
        input_window.transpose(1, 0, 2),
        write_window.transpose(1, 0, 2),
        read_window.transpose(1, 0, 2),
        ssm_state.reshape(rows, inner, STATE),
        out_gain,
    )
    lanes, packed, *staged = call(
        prepare_body,
        (
            pltpu.VMEM((8, inner), F32),
            pltpu.HBM((3 * width, block), BF16),
            pltpu.VMEM((width, 2 * inner), BF16),
            pltpu.VMEM((2 * latent + HEADS, width), BF16),
        )
        + tuple(pltpu.VMEM(v.shape, v.dtype) for v in staged),
        [SMEM] + [HBM] * (11 + STAGED),
        [
            pltpu.SMEM(step_bias.shape, F32),
            pltpu.SMEM(step_bias.shape, F32),
            pltpu.SMEM(step_bias.shape, F32),
            pltpu.VMEM((3 * width, block), BF16),
            pltpu.SemaphoreType.DMA((11 + pieces + STAGED,)),
        ],
        (VMEM, HBM) + (VMEM,) * (2 + STAGED),
    )(
        rank,
        *map(
            kept,
            (
                step_bias,
                decay_rate,
                skip_gain,
                expert_gate[0],
                expert_up[0],
                expert_down[0],
                *projections,
                *staged,
            ),
        ),
    )

    partial, new_state, new_input, new_write, new_read = call(
        mixer_body,
        (
            pltpu.HBM((tps, rows, width), BF16),
            sds((rows, inner, STATE), F32),
            sds((3, rows, inner), BF16),
            sds((3, rows, latent), BF16),
            sds((3, rows, latent), BF16),
        ),
        [SMEM] + [VMEM] * 14,
    )(rank, lanes, arrived, *staged, proj_out)
    mixed_in = lax.all_to_all(partial, "tp", 0, 0, tiled=True)
    ids, weights = expert_ids.T, expert_weights.T
    packed, ids, weights, _ = lax.optimization_barrier((packed, ids, weights, partial))
    select, combine = call(
        route_body,
        (
            sds((eps * pieces, rows * pieces), BF16),
            sds((4 * rows, 2 * tps * eps), BF16),
        ),
        [SMEM, HBM, HBM],
        [
            pltpu.VMEM(ids.shape, ids.dtype),
            pltpu.VMEM(weights.shape, F32),
            pltpu.SemaphoreType.DMA((2,)),
        ],
    )(rank, kept(ids), kept(weights))
    other = lax.ppermute(packed, "tp", [(t, t ^ 1) for t in range(tps)])

    outgoing, normed_ffn, hidden_part = call(
        hidden_body,
        (
            pltpu.HBM((eps * pieces, 128), BF16),
            sds((rows, width), BF16),
            sds((rows, quarter), BF16),
        ),
        [SMEM] + [VMEM] * 4,
        [pltpu.VMEM((rows * pieces, 128), F32)],
    )(rank, arrived, mixed_in, ffn_gain, select)
    items = lax.all_to_all(outgoing.reshape(eps, pieces, 128), "ep", 0, 0, tiled=True)

    give, keep, branch = call(
        dense_body,
        (sds((rows, width // 2), BF16), sds((rows, width // 2), BF16), sds((rows, 128), F32)),
        [SMEM] + [VMEM] * 5,
    )(rank, normed_ffn, dense_gate, dense_up, dense_down, branch_gate)
    got = lax.ppermute(give, "tp", [(t, t ^ 2) for t in range(tps)])
    give, left = call(
        halve_body, (sds((rows, quarter), BF16), sds((rows, quarter), F32)), [SMEM] + [VMEM] * 2
    )(rank, keep, got)
    items, give = lax.optimization_barrier((items, give))
    got = lax.ppermute(give, "tp", [(t, t ^ 1) for t in range(tps)])

    results = call(
        expert_body,
        pltpu.HBM((tps * eps * 2, 128), BF16),
        [VMEM] * 5,
        [pltpu.VMEM((eps * pieces, 128), F32), pltpu.VMEM((tps * eps * 2, 128), F32)],
    )(items.reshape(eps * pieces, 128), expert_gate[0], expert_up[0], expert_down[0], other)
    returned = lax.all_to_all(
        results.reshape(tps * eps, 2, 128), ("tp", "ep"), 0, 0, tiled=True
    ).reshape(tps * eps * 2, 128)

    new_hidden = call(final_body, sds((rows, quarter), BF16), [VMEM] * 6)(
        returned, combine, left, got, branch, hidden_part
    )
    return (
        new_hidden,
        new_state.reshape(rows, heads, HEAD_DIM, STATE),
        new_input.transpose(1, 0, 2),
        new_write.transpose(1, 0, 2),
        new_read.transpose(1, 0, 2),
    )


def solution(mesh):
    in_specs = (
        P("ep", "tp"),
        P("ep", None, "tp"),
        P("ep", None, "tp"),
        P("ep", None, "tp"),
        P("ep", "tp", None, None),
        P(),
        P(None, "tp"),
        P(None, "tp"),
        P(None, "tp"),
        P(None, "tp"),
        P(),
        P(None, "tp"),
        P(None, "tp"),
        P(None, "tp"),
        P(),
        P(),
        P(),
        P("tp"),
        P("tp", None),
        P(),
        P("ep", None),
        P("ep", None),
        P("ep", None, "tp"),
        P("ep", None, "tp"),
        P("ep", "tp", None),
        P(None, "tp"),
        P(None, "tp"),
        P(None, "tp"),
        P(),
    )
    out_specs = (
        P("ep", "tp"),
        P("ep", "tp", None, None),
        P("ep", None, "tp"),
        P("ep", None, "tp"),
        P("ep", None, "tp"),
    )
    return jax.shard_map(local, mesh=mesh, in_specs=in_specs, out_specs=out_specs, check_vma=False)
```

```python
import jax
import jax.numpy as jnp
from jax import lax
from jax.experimental import pallas as pl
from jax.experimental.pallas import tpu as pltpu
from jax.sharding import PartitionSpec as P


HEADS = 8
HEAD_DIM = 64
STATE = 64
EPS = 1e-06
F32 = jnp.float32
BF16 = jnp.bfloat16

HBM = pl.BlockSpec(memory_space=pltpu.HBM)
VMEM = pl.BlockSpec(memory_space=pltpu.VMEM)
SMEM = pl.BlockSpec(memory_space=pltpu.SMEM)
INTERPRET = False
LIMIT = 16 * 1024 * 1024


def call(body, outs, specs, scratch=(), out_spec=VMEM):
    return pl.pallas_call(
        body,
        out_shape=outs,
        in_specs=specs,
        out_specs=out_spec
        if isinstance(out_spec, tuple)
        else jax.tree.map(lambda _: out_spec, outs),
        scratch_shapes=scratch,
        compiler_params=pltpu.CompilerParams(vmem_limit_bytes=LIMIT),
        interpret=INTERPRET,
    )


def kept(value):
    return pltpu.with_memory_space_constraint(value, pltpu.HBM)


def sds(shape, dtype):
    return jax.ShapeDtypeStruct(shape, dtype)


def nt(a, b):
    return lax.dot_general(a, b, (((1,), (1,)), ((), ())), preferred_element_type=F32)


def nn(a, b):
    return jnp.dot(a, b, preferred_element_type=F32)


def silu(v):
    return v / (1.0 + jnp.exp(-v))


def softplus(v):
    return jnp.maximum(v, 0.0) + jnp.log1p(jnp.exp(-jnp.abs(v)))


def spread_body(tokens, out, here, sems):
    first = pltpu.make_async_copy(tokens, here, sems.at[out.shape[0]])
    first.start()
    first.wait()
    copies = [pltpu.make_async_copy(here, out.at[j], sems.at[j]) for j in range(out.shape[0])]
    for copy in copies:
        copy.start()
    for copy in copies:
        copy.wait()


def zeros_and_ones(shape, test):
    across = lax.broadcasted_iota(jnp.int32, shape, 1)
    down = lax.broadcasted_iota(jnp.int32, shape, 0)
    return test(down, across).astype(F32).astype(BF16)


def places(ids, experts):
    tops, rows = ids.shape
    expert = lax.broadcasted_iota(jnp.int32, (experts, rows), 0)
    same = [expert == ids[k : k + 1, :] for k in range(tops)]
    hits = jnp.zeros((experts, rows), F32)
    for match in same:
        hits = jnp.where(match, 1.0, hits)
    earlier = zeros_and_ones((rows, rows), lambda d, a: d < a)
    return same, hits, nn(hits.astype(BF16), earlier)


def selection(rank, ids, experts, pieces):
    rows = ids.shape[1]
    _, hits, place = places(ids, experts)
    mine = jnp.bitwise_and(rank[0], 1).astype(F32)
    chosen = jnp.where(place == mine, hits, 0.0).astype(BF16)
    down = zeros_and_ones((experts * pieces, experts), lambda d, a: d // pieces == a)
    across = zeros_and_ones((rows, rows * pieces), lambda d, a: a // pieces == d)
    wide = nn(down, nn(chosen, across).astype(BF16))
    matched = zeros_and_ones(wide.shape, lambda d, a: d % pieces == a % pieces)
    return wide.astype(BF16) * matched


def weigh_body(ids, weights, combine):
    tops, rows = ids.shape
    experts = combine.shape[1] // 8
    same, _, place = places(ids, experts)
    amount = jnp.zeros((experts, rows), F32)
    for k in range(tops):
        amount = jnp.where(same[k], weights[k : k + 1, :], amount)
    twice = zeros_and_ones((experts, experts * 2), lambda d, a: a // 2 == d)
    halves = lax.broadcasted_iota(jnp.int32, (rows, experts * 2), 1) % 2
    for s in range(2):
        part = jnp.where(place == float(s), amount, 0.0).T
        high = part.astype(BF16)
        low = (part - high.astype(F32)).astype(BF16)
        for p, piece in enumerate((high, low)):
            both = nn(piece, twice)
            for h in range(2):
                rows_at = (2 * p + h) * rows
                kept_half = jnp.where(halves == h, both, 0.0).astype(BF16)
                for t in (s, s + 2):
                    combine[
                        rows_at : rows_at + rows, t * 2 * experts : (t + 1) * 2 * experts
                    ] = kept_half


STAGED = 9


def prepare_body(*refs):
    rank, bias, rate, skip, gate, up, down = refs[:7]
    proj_gate, proj_input, proj_write, proj_read, proj_step = refs[7:12]
    sources = refs[12 : 12 + STAGED]
    lanes, packed, across, along = refs[12 + STAGED : 16 + STAGED]
    targets = refs[16 + STAGED : 16 + 2 * STAGED]
    bias_here, rate_here, skip_here, built, sems = refs[16 + 2 * STAGED :]
    width, block = gate.shape
    inner = proj_gate.shape[1]
    latent = proj_write.shape[0]
    pairs = [
        (bias, bias_here),
        (rate, rate_here),
        (skip, skip_here),
    ]
    pairs += [(gate, built.at[0:width]), (up, built.at[width : 2 * width])]
    for j in range(width // block):
        first = 2 * width + j * block
        pairs.append((down.at[:, j * block : (j + 1) * block], built.at[first : first + block]))
    building = len(pairs)
    pairs += [
        (proj_gate, across.at[:, 0:inner]),
        (proj_input, across.at[:, inner : 2 * inner]),
        (proj_write, along.at[0:latent]),
        (proj_read, along.at[latent : 2 * latent]),
        (proj_step, along.at[2 * latent : 2 * latent + HEADS]),
    ]
    pairs += list(zip(sources, targets))
    copies = [pltpu.make_async_copy(a, b, sems.at[k]) for k, (a, b) in enumerate(pairs)]
    out_copy = pltpu.make_async_copy(built, packed, sems.at[len(pairs)])
    for copy in copies:
        copy.start()
    for copy in copies[:building]:
        copy.wait()
    out_copy.start()
    heads = inner // HEAD_DIM
    lane_head = lax.broadcasted_iota(jnp.int32, (1, inner), 1) // HEAD_DIM
    for k, table in enumerate((bias_here, rate_here, skip_here)):
        line = jnp.zeros((1, inner), F32)
        for h in range(heads):
            line = jnp.where(lane_head == h, table[rank[0] * heads + h], line)
        lanes[k : k + 1, :] = line
    for copy in copies[building:]:
        copy.wait()
    out_copy.wait()


def conv(window, newest, taps, out_window):
    taken = taps[...].astype(F32)
    total = newest.astype(F32) * taken[3:4]
    for k in range(3):
        total += window[k].astype(F32) * taken[k : k + 1]
    out_window[0] = window[1]
    out_window[1] = window[2]
    out_window[2] = newest
    return silu(total)


def mixer_body(
    rank,
    lanes,
    arrived,
    across,
    along,
    norm_gain,
    taps_input,
    taps_write,
    taps_read,
    input_window,
    write_window,
    read_window,
    state,
    out_gain,
    proj_out,
    partial,
    new_state,
    new_input_window,
    new_write_window,
    new_read_window,
    fresh_state,
    sems,
):
    rows = arrived.shape[1]
    x = jnp.concatenate([arrived[j] for j in range(arrived.shape[0])], axis=1).astype(F32)
    scale = lax.rsqrt(jnp.mean(x * x, axis=-1, keepdims=True) + EPS)
    normed = (x * scale * norm_gain[...].astype(F32)[None, :]).astype(BF16)
    inner = input_window.shape[2]
    latent = write_window.shape[2]
    first = nn(normed, across[...])
    second = nt(normed, along[...])
    gate_rows = first[:, 0:inner].astype(BF16)
    input_rows = first[:, inner : 2 * inner].astype(BF16)
    write_rows = second[:, 0:latent].astype(BF16)
    read_rows = second[:, latent : 2 * latent].astype(BF16)
    step_all = second[:, 2 * latent : 2 * latent + HEADS]
    input_conv = conv(input_window, input_rows, taps_input, new_input_window)
    write_conv = conv(write_window, write_rows, taps_write, new_write_window)
    read_conv = conv(read_window, read_rows, taps_read, new_read_window)
    heads = inner // HEAD_DIM
    lane_head = lax.broadcasted_iota(jnp.int32, (rows, inner), 1) // HEAD_DIM
    column = lax.broadcasted_iota(jnp.int32, step_all.shape, 1)
    raw = jnp.zeros((rows, inner), F32)
    for h in range(heads):
        mine = column == rank[0] * heads + h
        raw = jnp.where(
            lane_head == h, jnp.sum(jnp.where(mine, step_all, 0.0), axis=1, keepdims=True), raw
        )
    step = softplus(raw + lanes[0:1, :])
    decay = jnp.exp(-step * lanes[1:2, :])
    scaled_t = (step * input_conv).T
    decay_t = decay.T
    lane = lax.broadcasted_iota(jnp.int32, (inner, rows), 1)
    readout_t = jnp.zeros((inner, rows), F32)
    for b in range(rows):
        fresh = (
            decay_t[:, b : b + 1] * state[b] + scaled_t[:, b : b + 1] * write_conv[b : b + 1, :]
        )
        fresh_state[b] = fresh
        seen = jnp.sum(fresh * read_conv[b : b + 1, :], axis=1, keepdims=True)
        readout_t = jnp.where(lane == b, seen, readout_t)
    state_copy = pltpu.make_async_copy(fresh_state, new_state, sems.at[0])
    state_copy.start()
    readout = readout_t.T + lanes[2:3, :] * input_conv
    gated = readout * silu(gate_rows.astype(F32))
    gated = gated * lax.rsqrt(jnp.mean(gated * gated, axis=-1, keepdims=True) + EPS)
    mixer_rows = (gated * out_gain[...].astype(F32)[None, :]).astype(BF16)
    mixed = nn(mixer_rows, proj_out[...]).astype(BF16)
    for j in range(partial.shape[0]):
        partial[j] = mixed
    state_copy.wait()


def hidden_body(
    rank, arrived, mixed_in, ffn_gain, ids, outgoing, normed_out, hidden_part, folded
):
    count, rows, quarter = arrived.shape
    pieces = folded.shape[0] // rows
    select = selection(rank, ids, outgoing.shape[0] // pieces, pieces)
    x = jnp.concatenate([arrived[j] for j in range(count)], axis=1).astype(F32)
    mixed = mixed_in[0].astype(F32)
    for j in range(1, count):
        mixed += mixed_in[j].astype(F32)
    hidden = (x + mixed).astype(BF16)
    wide = hidden.astype(F32)
    scale = lax.rsqrt(jnp.mean(wide * wide, axis=-1, keepdims=True) + EPS)
    normed_wide = wide * scale * ffn_gain[...].astype(F32)[None, :]
    normed_out[...] = normed_wide.astype(BF16)
    for j in range(pieces):
        folded[pl.ds(j, rows, stride=pieces), :] = normed_wide[:, j * 128 : (j + 1) * 128]
    outgoing[...] = nn(select, folded[...].astype(BF16)).astype(BF16)
    part = wide[:, 0:quarter]
    for j in range(1, count):
        part = jnp.where(rank[0] == j, wide[:, j * quarter : (j + 1) * quarter], part)
    hidden_part[...] = part.astype(BF16)


def dense_body(rank, normed_in, gate, up, down, branch_gate, give, keep, branch):
    normed = normed_in[...]
    hidden = (silu(nn(normed, gate[...])) * nn(normed, up[...])).astype(BF16)
    total = nt(hidden, down[...]).astype(BF16)
    half = give.shape[1]
    upper = rank[0] > 1
    give[...] = jnp.where(upper, total[:, 0:half], total[:, half:])
    keep[...] = jnp.where(upper, total[:, half:], total[:, 0:half])
    level = jnp.sum(
        normed.astype(F32) * branch_gate[...].astype(F32)[None, :], axis=-1, keepdims=True
    )
    branch[...] = jnp.broadcast_to(jax.nn.sigmoid(level), branch.shape)


def halve_body(rank, keep, got, give, left):
    total = keep[...].astype(F32) + got[...].astype(F32)
    quarter = give.shape[1]
    odd = jnp.bitwise_and(rank[0], 1) > 0
    give[...] = jnp.where(odd, total[:, 0:quarter], total[:, quarter:]).astype(BF16)
    left[...] = jnp.where(odd, total[:, quarter:], total[:, 0:quarter])


def expert_body(items, gate, up, down, other, out, unfolded, fold):
    width, block = gate.shape
    pieces = width // 128
    count = items.shape[0] // pieces
    unfolded[...] = items[...].astype(F32)
    x = jnp.concatenate(
        [unfolded[pl.ds(j, count, stride=pieces), :].astype(BF16) for j in range(pieces)], axis=1
    )
    act = (silu(nn(x, gate[...])) * nn(x, up[...])).astype(BF16)
    act_other = (silu(nn(x, other[0:width])) * nn(x, other[width : 2 * width])).astype(BF16)
    total = nn(act, down[...])
    for j in range(pieces):
        first = 2 * width + j * block
        piece = total[:, j * block : (j + 1) * block] + nn(act_other, other[first : first + block])
        fold[pl.ds(j // 2 * 2 * count + j % 2, count, stride=2), :] = piece
    out[...] = fold[...].astype(BF16)


def final_body(returned, combine, left, got, branch, hidden_part, out):
    total = hidden_part[...].astype(F32)
    rows = total.shape[0]
    dense = left[...] + got[...].astype(F32)
    sums = nn(combine[...], returned[...])
    sums = sums[0 : 2 * rows] + sums[2 * rows :]
    total += jnp.concatenate([sums[0:rows], sums[rows:]], axis=1)
    total += branch[:, 0:1] * dense
    out[...] = total.astype(BF16)


def local(
    tokens,
    input_window,
    write_window,
    read_window,
    ssm_state,
    norm_gain,
    proj_gate,
    proj_input,
    proj_write,
    proj_read,
    proj_step,
    taps_input,
    taps_write,
    taps_read,
    step_bias,
    decay_rate,
    skip_gain,
    out_gain,
    proj_out,
    ffn_gain,
    expert_ids,
    expert_weights,
    expert_gate,
    expert_up,
    expert_down,
    dense_gate,
    dense_up,
    dense_down,
    branch_gate,
):
    tps = lax.axis_size("tp")
    eps = lax.axis_size("ep")
    rank = lax.axis_index("tp").astype(jnp.int32).reshape(1)
    rows, quarter = tokens.shape
    width = quarter * tps
    inner = proj_gate.shape[1]
    latent = proj_write.shape[1]
    heads = ssm_state.shape[1]
    block = expert_gate.shape[2]

    pieces = width // 128

    spread = call(
        spread_body,
        sds((tps, rows, quarter), BF16),
        [HBM],
        [pltpu.VMEM((rows, quarter), BF16), pltpu.SemaphoreType.DMA((tps + 1,))],
        HBM,
    )(kept(tokens))
    arrived = lax.all_to_all(spread, "tp", 0, 0, tiled=True)

    projections = (proj_gate, proj_input, proj_write.T, proj_read.T, proj_step.T)
    staged = (
        norm_gain,
        taps_input,
        taps_write,
        taps_read,
        input_window.transpose(1, 0, 2),
        write_window.transpose(1, 0, 2),
        read_window.transpose(1, 0, 2),
        ssm_state.reshape(rows, inner, STATE),
        out_gain,
    )
    lanes, packed, *staged = call(
        prepare_body,
        (
            pltpu.VMEM((8, inner), F32),
            pltpu.HBM((3 * width, block), BF16),
            pltpu.VMEM((width, 2 * inner), BF16),
            pltpu.VMEM((2 * latent + HEADS, width), BF16),
        )
        + tuple(pltpu.VMEM(v.shape, v.dtype) for v in staged),
        [SMEM] + [HBM] * (11 + STAGED),
        [
            pltpu.SMEM(step_bias.shape, F32),
            pltpu.SMEM(step_bias.shape, F32),
            pltpu.SMEM(step_bias.shape, F32),
            pltpu.VMEM((3 * width, block), BF16),
            pltpu.SemaphoreType.DMA((11 + pieces + STAGED,)),
        ],
        (VMEM, HBM) + (VMEM,) * (2 + STAGED),
    )(
        rank,
        *map(
            kept,
            (
                step_bias,
                decay_rate,
                skip_gain,
                expert_gate[0],
                expert_up[0],
                expert_down[0],
                *projections,
                *staged,
            ),
        ),
    )

    partial, new_state, new_input, new_write, new_read = call(
        mixer_body,
        (
            pltpu.HBM((tps, rows, width), BF16),
            sds((rows, inner, STATE), F32),
            sds((3, rows, inner), BF16),
            sds((3, rows, latent), BF16),
            sds((3, rows, latent), BF16),
        ),
        [SMEM] + [VMEM] * 14,
        [pltpu.VMEM((rows, inner, STATE), F32), pltpu.SemaphoreType.DMA((1,))],
        (VMEM, HBM, VMEM, VMEM, VMEM),
    )(rank, lanes, arrived, *staged, proj_out)
    mixed_in = lax.all_to_all(partial, "tp", 0, 0, tiled=True)
    packed, _ = lax.optimization_barrier((packed, partial))
    other = lax.ppermute(packed, "tp", [(t, t ^ 1) for t in range(tps)])

    outgoing, normed_ffn, hidden_part = call(
        hidden_body,
        (
            pltpu.HBM((eps * pieces, 128), BF16),
            sds((rows, width), BF16),
            sds((rows, quarter), BF16),
        ),
        [SMEM] + [VMEM] * 4,
        [pltpu.VMEM((rows * pieces, 128), F32)],
    )(rank, arrived, mixed_in, ffn_gain, expert_ids.T)
    items = lax.all_to_all(outgoing.reshape(eps, pieces, 128), "ep", 0, 0, tiled=True)

    ids, weights, normed_ffn = lax.optimization_barrier(
        (expert_ids.T, expert_weights.T, normed_ffn)
    )
    combine = call(weigh_body, sds((4 * rows, 2 * tps * eps), BF16), [VMEM] * 2)(ids, weights)
    give, keep, branch = call(
        dense_body,
        (sds((rows, width // 2), BF16), sds((rows, width // 2), BF16), sds((rows, 128), F32)),
        [SMEM] + [VMEM] * 5,
    )(rank, normed_ffn, dense_gate, dense_up, dense_down, branch_gate)
    got = lax.ppermute(give, "tp", [(t, t ^ 2) for t in range(tps)])
    give, left = call(
        halve_body, (sds((rows, quarter), BF16), sds((rows, quarter), F32)), [SMEM] + [VMEM] * 2
    )(rank, keep, got)
    items, give = lax.optimization_barrier((items, give))
    got = lax.ppermute(give, "tp", [(t, t ^ 1) for t in range(tps)])

    results = call(
        expert_body,
        pltpu.HBM((tps * eps * 2, 128), BF16),
        [VMEM] * 5,
        [pltpu.VMEM((eps * pieces, 128), F32), pltpu.VMEM((tps * eps * 2, 128), F32)],
    )(items.reshape(eps * pieces, 128), expert_gate[0], expert_up[0], expert_down[0], other)
    returned = lax.all_to_all(
        results.reshape(tps * eps, 2, 128), ("tp", "ep"), 0, 0, tiled=True
    ).reshape(tps * eps * 2, 128)

    new_hidden = call(final_body, sds((rows, quarter), BF16), [VMEM] * 6)(
        returned, combine, left, got, branch, hidden_part
    )
    return (
        new_hidden,
        new_state.reshape(rows, heads, HEAD_DIM, STATE),
        new_input.transpose(1, 0, 2),
        new_write.transpose(1, 0, 2),
        new_read.transpose(1, 0, 2),
    )


def solution(mesh):
    in_specs = (
        P("ep", "tp"),
        P("ep", None, "tp"),
        P("ep", None, "tp"),
        P("ep", None, "tp"),
        P("ep", "tp", None, None),
        P(),
        P(None, "tp"),
        P(None, "tp"),
        P(None, "tp"),
        P(None, "tp"),
        P(),
        P(None, "tp"),
        P(None, "tp"),
        P(None, "tp"),
        P(),
        P(),
        P(),
        P("tp"),
        P("tp", None),
        P(),
        P("ep", None),
        P("ep", None),
        P("ep", None, "tp"),
        P("ep", None, "tp"),
        P("ep", "tp", None),
        P(None, "tp"),
        P(None, "tp"),
        P(None, "tp"),
        P(),
    )
    out_specs = (
        P("ep", "tp"),
        P("ep", "tp", None, None),
        P("ep", None, "tp"),
        P("ep", None, "tp"),
        P("ep", None, "tp"),
    )
    return jax.shard_map(local, mesh=mesh, in_specs=in_specs, out_specs=out_specs, check_vma=False)
```

```python
import jax
import jax.numpy as jnp
from jax import lax
from jax.experimental import pallas as pl
from jax.experimental.pallas import tpu as pltpu
from jax.sharding import PartitionSpec as P


HEADS = 8
HEAD_DIM = 64
STATE = 64
EPS = 1e-06
F32 = jnp.float32
BF16 = jnp.bfloat16

HBM = pl.BlockSpec(memory_space=pltpu.HBM)
VMEM = pl.BlockSpec(memory_space=pltpu.VMEM)
SMEM = pl.BlockSpec(memory_space=pltpu.SMEM)
INTERPRET = False
LIMIT = 16 * 1024 * 1024


def call(body, outs, specs, scratch=(), out_spec=VMEM):
    return pl.pallas_call(
        body,
        out_shape=outs,
        in_specs=specs,
        out_specs=out_spec
        if isinstance(out_spec, tuple)
        else jax.tree.map(lambda _: out_spec, outs),
        scratch_shapes=scratch,
        compiler_params=pltpu.CompilerParams(vmem_limit_bytes=LIMIT),
        interpret=INTERPRET,
    )


def kept(value):
    return pltpu.with_memory_space_constraint(value, pltpu.HBM)


def sds(shape, dtype):
    return jax.ShapeDtypeStruct(shape, dtype)


def nt(a, b):
    return lax.dot_general(a, b, (((1,), (1,)), ((), ())), preferred_element_type=F32)


def nn(a, b):
    return jnp.dot(a, b, preferred_element_type=F32)


def silu(v):
    return v / (1.0 + jnp.exp(-v))


def softplus(v):
    return jnp.maximum(v, 0.0) + jnp.log1p(jnp.exp(-jnp.abs(v)))


def spread_body(tokens, out, here, sems):
    first = pltpu.make_async_copy(tokens, here, sems.at[out.shape[0]])
    first.start()
    first.wait()
    copies = [pltpu.make_async_copy(here, out.at[j], sems.at[j]) for j in range(out.shape[0])]
    for copy in copies:
        copy.start()
    for copy in copies:
        copy.wait()


def zeros_and_ones(shape, test):
    across = lax.broadcasted_iota(jnp.int32, shape, 1)
    down = lax.broadcasted_iota(jnp.int32, shape, 0)
    return test(down, across).astype(F32).astype(BF16)


def places(ids, experts):
    tops, rows = ids.shape
    expert = lax.broadcasted_iota(jnp.int32, (experts, rows), 0)
    same = [expert == ids[k : k + 1, :] for k in range(tops)]
    hits = jnp.zeros((experts, rows), F32)
    for match in same:
        hits = jnp.where(match, 1.0, hits)
    earlier = zeros_and_ones((rows, rows), lambda d, a: d < a)
    return same, hits, nn(hits.astype(BF16), earlier)


def select_body(rank, ids, select):
    rows = ids.shape[1]
    pieces = select.shape[1] // rows
    experts = select.shape[0] // pieces
    _, hits, place = places(ids, experts)
    mine = jnp.bitwise_and(rank[0], 1).astype(F32)
    chosen = jnp.where(place == mine, hits, 0.0).astype(BF16)
    down = zeros_and_ones((experts * pieces, experts), lambda d, a: d // pieces == a)
    across = zeros_and_ones((rows, rows * pieces), lambda d, a: a // pieces == d)
    wide = nn(down, nn(chosen, across).astype(BF16))
    matched = zeros_and_ones(wide.shape, lambda d, a: d % pieces == a % pieces)
    select[...] = wide.astype(BF16) * matched


def weigh_body(ids, weights, normed, branch_gate, combine, branch):
    tops, rows = ids.shape
    experts = combine.shape[1] // 8
    same, _, place = places(ids, experts)
    amount = jnp.zeros((experts, rows), F32)
    for k in range(tops):
        amount = jnp.where(same[k], weights[k : k + 1, :], amount)
    twice = zeros_and_ones((experts, experts * 2), lambda d, a: a // 2 == d)
    halves = lax.broadcasted_iota(jnp.int32, (rows, experts * 2), 1) % 2
    for s in range(2):
        part = jnp.where(place == float(s), amount, 0.0).T
        high = part.astype(BF16)
        low = (part - high.astype(F32)).astype(BF16)
        for p, piece in enumerate((high, low)):
            both = nn(piece, twice)
            for h in range(2):
                rows_at = (2 * p + h) * rows
                kept_half = jnp.where(halves == h, both, 0.0).astype(BF16)
                for t in (s, s + 2):
                    combine[
                        rows_at : rows_at + rows, t * 2 * experts : (t + 1) * 2 * experts
                    ] = kept_half
    scaled = normed[...].astype(F32) * branch_gate[...].astype(F32)[None, :]
    level = jnp.sum(scaled, axis=-1, keepdims=True)
    branch[...] = jnp.broadcast_to(jax.nn.sigmoid(level), branch.shape)


STAGED = 9


def prepare_body(*refs):
    rank, bias, rate, skip, gate, up, down = refs[:7]
    proj_gate, proj_input, proj_write, proj_read, proj_step = refs[7:12]
    sources = refs[12 : 12 + STAGED]
    lanes, packed, across, along = refs[12 + STAGED : 16 + STAGED]
    targets = refs[16 + STAGED : 16 + 2 * STAGED]
    bias_here, rate_here, skip_here, built, sems = refs[16 + 2 * STAGED :]
    width, block = gate.shape
    inner = proj_gate.shape[1]
    latent = proj_write.shape[0]
    pairs = [
        (bias, bias_here),
        (rate, rate_here),
        (skip, skip_here),
    ]
    pairs += [(gate, built.at[0:width]), (up, built.at[width : 2 * width])]
    for j in range(width // block):
        first = 2 * width + j * block
        pairs.append((down.at[:, j * block : (j + 1) * block], built.at[first : first + block]))
    building = len(pairs)
    pairs += [
        (proj_gate, across.at[:, 0:inner]),
        (proj_input, across.at[:, inner : 2 * inner]),
        (proj_write, along.at[0:latent]),
        (proj_read, along.at[latent : 2 * latent]),
        (proj_step, along.at[2 * latent : 2 * latent + HEADS]),
    ]
    pairs += list(zip(sources, targets))
    copies = [pltpu.make_async_copy(a, b, sems.at[k]) for k, (a, b) in enumerate(pairs)]
    out_copy = pltpu.make_async_copy(built, packed, sems.at[len(pairs)])
    for copy in copies:
        copy.start()
    for copy in copies[:building]:
        copy.wait()
    out_copy.start()
    heads = inner // HEAD_DIM
    lane_head = lax.broadcasted_iota(jnp.int32, (1, inner), 1) // HEAD_DIM
    for k, table in enumerate((bias_here, rate_here, skip_here)):
        line = jnp.zeros((1, inner), F32)
        for h in range(heads):
            line = jnp.where(lane_head == h, table[rank[0] * heads + h], line)
        lanes[k : k + 1, :] = line
    for copy in copies[building:]:
        copy.wait()
    out_copy.wait()


def conv(window, newest, taps, out_window):
    taken = taps[...].astype(F32)
    total = newest.astype(F32) * taken[3:4]
    for k in range(3):
        total += window[k].astype(F32) * taken[k : k + 1]
    out_window[0] = window[1]
    out_window[1] = window[2]
    out_window[2] = newest
    return silu(total)


def mixer_body(
    rank,
    lanes,
    arrived,
    across,
    along,
    norm_gain,
    taps_input,
    taps_write,
    taps_read,
    input_window,
    write_window,
    read_window,
    state,
    out_gain,
    proj_out,
    partial,
    new_state,
    new_input_window,
    new_write_window,
    new_read_window,
):
    rows = arrived.shape[1]
    x = jnp.concatenate([arrived[j] for j in range(arrived.shape[0])], axis=1).astype(F32)
    scale = lax.rsqrt(jnp.mean(x * x, axis=-1, keepdims=True) + EPS)
    normed = (x * scale * norm_gain[...].astype(F32)[None, :]).astype(BF16)
    inner = input_window.shape[2]
    latent = write_window.shape[2]
    first = nn(normed, across[...])
    second = nt(normed, along[...])
    gate_rows = first[:, 0:inner].astype(BF16)
    input_rows = first[:, inner : 2 * inner].astype(BF16)
    write_rows = second[:, 0:latent].astype(BF16)
    read_rows = second[:, latent : 2 * latent].astype(BF16)
    step_all = second[:, 2 * latent : 2 * latent + HEADS]
    input_conv = conv(input_window, input_rows, taps_input, new_input_window)
    write_conv = conv(write_window, write_rows, taps_write, new_write_window)
    read_conv = conv(read_window, read_rows, taps_read, new_read_window)
    heads = inner // HEAD_DIM
    lane_head = lax.broadcasted_iota(jnp.int32, (rows, inner), 1) // HEAD_DIM
    column = lax.broadcasted_iota(jnp.int32, step_all.shape, 1)
    raw = jnp.zeros((rows, inner), F32)
    for h in range(heads):
        mine = column == rank[0] * heads + h
        raw = jnp.where(
            lane_head == h, jnp.sum(jnp.where(mine, step_all, 0.0), axis=1, keepdims=True), raw
        )
    step = softplus(raw + lanes[0:1, :])
    decay = jnp.exp(-step * lanes[1:2, :])
    scaled_t = (step * input_conv).T
    decay_t = decay.T
    lane = lax.broadcasted_iota(jnp.int32, (inner, rows), 1)
    readout_t = jnp.zeros((inner, rows), F32)
    for b in range(rows):
        fresh = (
            decay_t[:, b : b + 1] * state[b] + scaled_t[:, b : b + 1] * write_conv[b : b + 1, :]
        )
        new_state[b] = fresh
        seen = jnp.sum(fresh * read_conv[b : b + 1, :], axis=1, keepdims=True)
        readout_t = jnp.where(lane == b, seen, readout_t)
    readout = readout_t.T + lanes[2:3, :] * input_conv
    gated = readout * silu(gate_rows.astype(F32))
    gated = gated * lax.rsqrt(jnp.mean(gated * gated, axis=-1, keepdims=True) + EPS)
    mixer_rows = (gated * out_gain[...].astype(F32)[None, :]).astype(BF16)
    mixed = nn(mixer_rows, proj_out[...]).astype(BF16)
    for j in range(partial.shape[0]):
        partial[j] = mixed


def hidden_body(
    rank, arrived, mixed_in, ffn_gain, select, outgoing, normed_out, hidden_part, folded
):
    count, rows, quarter = arrived.shape
    pieces = folded.shape[0] // rows
    x = jnp.concatenate([arrived[j] for j in range(count)], axis=1).astype(F32)
    mixed = mixed_in[0].astype(F32)
    for j in range(1, count):
        mixed += mixed_in[j].astype(F32)
    hidden = (x + mixed).astype(BF16)
    wide = hidden.astype(F32)
    scale = lax.rsqrt(jnp.mean(wide * wide, axis=-1, keepdims=True) + EPS)
    normed_wide = wide * scale * ffn_gain[...].astype(F32)[None, :]
    normed_out[...] = normed_wide.astype(BF16)
    for j in range(pieces):
        folded[pl.ds(j, rows, stride=pieces), :] = normed_wide[:, j * 128 : (j + 1) * 128]
    outgoing[...] = nn(select[...], folded[...].astype(BF16)).astype(BF16)
    part = wide[:, 0:quarter]
    for j in range(1, count):
        part = jnp.where(rank[0] == j, wide[:, j * quarter : (j + 1) * quarter], part)
    hidden_part[...] = part.astype(BF16)


def dense_body(rank, normed_in, gate, up, down, give, keep):
    normed = normed_in[...]
    hidden = (silu(nn(normed, gate[...])) * nn(normed, up[...])).astype(BF16)
    total = nt(hidden, down[...]).astype(BF16)
    half = give.shape[1]
    upper = rank[0] > 1
    give[...] = jnp.where(upper, total[:, 0:half], total[:, half:])
    keep[...] = jnp.where(upper, total[:, half:], total[:, 0:half])


def halve_body(rank, keep, got, give, left):
    total = keep[...].astype(F32) + got[...].astype(F32)
    quarter = give.shape[1]
    odd = jnp.bitwise_and(rank[0], 1) > 0
    give[...] = jnp.where(odd, total[:, 0:quarter], total[:, quarter:]).astype(BF16)
    left[...] = jnp.where(odd, total[:, quarter:], total[:, 0:quarter])


def expert_body(items, gate, up, down, other, out, unfolded, fold):
    width, block = gate.shape
    pieces = width // 128
    count = items.shape[0] // pieces
    unfolded[...] = items[...].astype(F32)
    x = jnp.concatenate(
        [unfolded[pl.ds(j, count, stride=pieces), :].astype(BF16) for j in range(pieces)], axis=1
    )
    act = (silu(nn(x, gate[...])) * nn(x, up[...])).astype(BF16)
    act_other = (silu(nn(x, other[0:width])) * nn(x, other[width : 2 * width])).astype(BF16)
    total = nn(act, down[...])
    for j in range(pieces):
        first = 2 * width + j * block
        piece = total[:, j * block : (j + 1) * block] + nn(act_other, other[first : first + block])
        fold[pl.ds(j // 2 * 2 * count + j % 2, count, stride=2), :] = piece
    out[...] = fold[...].astype(BF16)


def final_body(returned, combine, left, got, branch, hidden_part, out):
    total = hidden_part[...].astype(F32)
    rows = total.shape[0]
    dense = left[...] + got[...].astype(F32)
    sums = nn(combine[...], returned[...])
    sums = sums[0 : 2 * rows] + sums[2 * rows :]
    total += jnp.concatenate([sums[0:rows], sums[rows:]], axis=1)
    total += branch[:, 0:1] * dense
    out[...] = total.astype(BF16)


def local(
    tokens,
    input_window,
    write_window,
    read_window,
    ssm_state,
    norm_gain,
    proj_gate,
    proj_input,
    proj_write,
    proj_read,
    proj_step,
    taps_input,
    taps_write,
    taps_read,
    step_bias,
    decay_rate,
    skip_gain,
    out_gain,
    proj_out,
    ffn_gain,
    expert_ids,
    expert_weights,
    expert_gate,
    expert_up,
    expert_down,
    dense_gate,
    dense_up,
    dense_down,
    branch_gate,
):
    tps = lax.axis_size("tp")
    eps = lax.axis_size("ep")
    rank = lax.axis_index("tp").astype(jnp.int32).reshape(1)
    rows, quarter = tokens.shape
    width = quarter * tps
    inner = proj_gate.shape[1]
    latent = proj_write.shape[1]
    heads = ssm_state.shape[1]
    block = expert_gate.shape[2]

    pieces = width // 128

    spread = call(
        spread_body,
        sds((tps, rows, quarter), BF16),
        [HBM],
        [pltpu.VMEM((rows, quarter), BF16), pltpu.SemaphoreType.DMA((tps + 1,))],
        HBM,
    )(kept(tokens))
    arrived = lax.all_to_all(spread, "tp", 0, 0, tiled=True)

    projections = (proj_gate, proj_input, proj_write.T, proj_read.T, proj_step.T)
    staged = (
        norm_gain,
        taps_input,
        taps_write,
        taps_read,
        input_window.transpose(1, 0, 2),
        write_window.transpose(1, 0, 2),
        read_window.transpose(1, 0, 2),
        ssm_state.reshape(rows, inner, STATE),
        out_gain,
    )
    lanes, packed, *staged = call(
        prepare_body,
        (
            pltpu.VMEM((8, inner), F32),
            pltpu.HBM((3 * width, block), BF16),
            pltpu.VMEM((width, 2 * inner), BF16),
            pltpu.VMEM((2 * latent + HEADS, width), BF16),
        )
        + tuple(pltpu.VMEM(v.shape, v.dtype) for v in staged),
        [SMEM] + [HBM] * (11 + STAGED),
        [
            pltpu.SMEM(step_bias.shape, F32),
            pltpu.SMEM(step_bias.shape, F32),
            pltpu.SMEM(step_bias.shape, F32),
            pltpu.VMEM((3 * width, block), BF16),
            pltpu.SemaphoreType.DMA((11 + pieces + STAGED,)),
        ],
        (VMEM, HBM) + (VMEM,) * (2 + STAGED),
    )(
        rank,
        *map(
            kept,
            (
                step_bias,
                decay_rate,
                skip_gain,
                expert_gate[0],
                expert_up[0],
                expert_down[0],
                *projections,
                *staged,
            ),
        ),
    )

    partial, new_state, new_input, new_write, new_read = call(
        mixer_body,
        (
            pltpu.HBM((tps, rows, width), BF16),
            sds((rows, inner, STATE), F32),
            sds((3, rows, inner), BF16),
            sds((3, rows, latent), BF16),
            sds((3, rows, latent), BF16),
        ),
        [SMEM] + [VMEM] * 14,
    )(rank, lanes, arrived, *staged, proj_out)
    mixed_in = lax.all_to_all(partial, "tp", 0, 0, tiled=True)
    packed, ids, _ = lax.optimization_barrier((packed, expert_ids.T, partial))
    select = call(select_body, sds((eps * pieces, rows * pieces), BF16), [SMEM, VMEM])(rank, ids)
    other = lax.ppermute(packed, "tp", [(t, t ^ 1) for t in range(tps)])

    outgoing, normed_ffn, hidden_part = call(
        hidden_body,
        (
            pltpu.HBM((eps * pieces, 128), BF16),
            sds((rows, width), BF16),
            sds((rows, quarter), BF16),
        ),
        [SMEM] + [VMEM] * 4,
        [pltpu.VMEM((rows * pieces, 128), F32)],
    )(rank, arrived, mixed_in, ffn_gain, select)
    items = lax.all_to_all(outgoing.reshape(eps, pieces, 128), "ep", 0, 0, tiled=True)

    ids, weights, gate_line, normed_ffn = lax.optimization_barrier(
        (expert_ids.T, expert_weights.T, branch_gate, normed_ffn)
    )
    combine, branch = call(
        weigh_body, (sds((4 * rows, 2 * tps * eps), BF16), sds((rows, 128), F32)), [VMEM] * 4
    )(ids, weights, normed_ffn, gate_line)
    give, keep = call(
        dense_body,
        (sds((rows, width // 2), BF16), sds((rows, width // 2), BF16)),
        [SMEM] + [VMEM] * 4,
    )(rank, normed_ffn, dense_gate, dense_up, dense_down)
    got = lax.ppermute(give, "tp", [(t, t ^ 2) for t in range(tps)])
    give, left = call(
        halve_body, (sds((rows, quarter), BF16), sds((rows, quarter), F32)), [SMEM] + [VMEM] * 2
    )(rank, keep, got)
    items, give = lax.optimization_barrier((items, give))
    got = lax.ppermute(give, "tp", [(t, t ^ 1) for t in range(tps)])

    results = call(
        expert_body,
        pltpu.HBM((tps * eps * 2, 128), BF16),
        [VMEM] * 5,
        [pltpu.VMEM((eps * pieces, 128), F32), pltpu.VMEM((tps * eps * 2, 128), F32)],
    )(items.reshape(eps * pieces, 128), expert_gate[0], expert_up[0], expert_down[0], other)
    returned = lax.all_to_all(
        results.reshape(tps * eps, 2, 128), ("tp", "ep"), 0, 0, tiled=True
    ).reshape(tps * eps * 2, 128)

    new_hidden = call(final_body, sds((rows, quarter), BF16), [VMEM] * 6)(
        returned, combine, left, got, branch, hidden_part
    )
    return (
        new_hidden,
        new_state.reshape(rows, heads, HEAD_DIM, STATE),
        new_input.transpose(1, 0, 2),
        new_write.transpose(1, 0, 2),
        new_read.transpose(1, 0, 2),
    )


def solution(mesh):
    in_specs = (
        P("ep", "tp"),
        P("ep", None, "tp"),
        P("ep", None, "tp"),
        P("ep", None, "tp"),
        P("ep", "tp", None, None),
        P(),
        P(None, "tp"),
        P(None, "tp"),
        P(None, "tp"),
        P(None, "tp"),
        P(),
        P(None, "tp"),
        P(None, "tp"),
        P(None, "tp"),
        P(),
        P(),
        P(),
        P("tp"),
        P("tp", None),
        P(),
        P("ep", None),
        P("ep", None),
        P("ep", None, "tp"),
        P("ep", None, "tp"),
        P("ep", "tp", None),
        P(None, "tp"),
        P(None, "tp"),
        P(None, "tp"),
        P(),
    )
    out_specs = (
        P("ep", "tp"),
        P("ep", "tp", None, None),
        P("ep", None, "tp"),
        P("ep", None, "tp"),
        P("ep", None, "tp"),
    )
    return jax.shard_map(local, mesh=mesh, in_specs=in_specs, out_specs=out_specs, check_vma=False)
```

```python
import jax
import jax.numpy as jnp
from jax import lax
from jax.experimental import pallas as pl
from jax.experimental.pallas import tpu as pltpu
from jax.sharding import PartitionSpec as P


HEADS = 8
HEAD_DIM = 64
STATE = 64
EPS = 1e-06
F32 = jnp.float32
BF16 = jnp.bfloat16

HBM = pl.BlockSpec(memory_space=pltpu.HBM)
VMEM = pl.BlockSpec(memory_space=pltpu.VMEM)
SMEM = pl.BlockSpec(memory_space=pltpu.SMEM)
INTERPRET = False
LIMIT = 16 * 1024 * 1024


def call(body, outs, specs, scratch=(), out_spec=VMEM):
    return pl.pallas_call(
        body,
        out_shape=outs,
        in_specs=specs,
        out_specs=out_spec
        if isinstance(out_spec, tuple)
        else jax.tree.map(lambda _: out_spec, outs),
        scratch_shapes=scratch,
        compiler_params=pltpu.CompilerParams(vmem_limit_bytes=LIMIT),
        interpret=INTERPRET,
    )


def kept(value):
    return pltpu.with_memory_space_constraint(value, pltpu.HBM)


def sds(shape, dtype):
    return jax.ShapeDtypeStruct(shape, dtype)


def nt(a, b):
    return lax.dot_general(a, b, (((1,), (1,)), ((), ())), preferred_element_type=F32)


def nn(a, b):
    return jnp.dot(a, b, preferred_element_type=F32)


def silu(v):
    return v / (1.0 + jnp.exp(-v))


def softplus(v):
    return jnp.maximum(v, 0.0) + jnp.log1p(jnp.exp(-jnp.abs(v)))


def spread_body(tokens, out, here, sems):
    first = pltpu.make_async_copy(tokens, here, sems.at[out.shape[0]])
    first.start()
    first.wait()
    copies = [pltpu.make_async_copy(here, out.at[j], sems.at[j]) for j in range(out.shape[0])]
    for copy in copies:
        copy.start()
    for copy in copies:
        copy.wait()


def zeros_and_ones(shape, test):
    across = lax.broadcasted_iota(jnp.int32, shape, 1)
    down = lax.broadcasted_iota(jnp.int32, shape, 0)
    return test(down, across).astype(F32).astype(BF16)


def places(ids, experts):
    tops, rows = ids.shape
    expert = lax.broadcasted_iota(jnp.int32, (experts, rows), 0)
    same = [expert == ids[k : k + 1, :] for k in range(tops)]
    hits = jnp.zeros((experts, rows), F32)
    for match in same:
        hits = jnp.where(match, 1.0, hits)
    earlier = zeros_and_ones((rows, rows), lambda d, a: d < a)
    return same, hits, nn(hits.astype(BF16), earlier)


def select_body(rank, ids, select):
    rows = ids.shape[1]
    pieces = select.shape[1] // rows
    experts = select.shape[0] // pieces
    _, hits, place = places(ids, experts)
    mine = jnp.bitwise_and(rank[0], 1).astype(F32)
    chosen = jnp.where(place == mine, hits, 0.0).astype(BF16)
    down = zeros_and_ones((experts * pieces, experts), lambda d, a: d // pieces == a)
    across = zeros_and_ones((rows, rows * pieces), lambda d, a: a // pieces == d)
    wide = nn(down, nn(chosen, across).astype(BF16))
    matched = zeros_and_ones(wide.shape, lambda d, a: d % pieces == a % pieces)
    select[...] = wide.astype(BF16) * matched


def weigh_body(ids, weights, normed, branch_gate, combine, branch):
    tops, rows = ids.shape
    experts = combine.shape[1] // 8
    same, _, place = places(ids, experts)
    amount = jnp.zeros((experts, rows), F32)
    for k in range(tops):
        amount = jnp.where(same[k], weights[k : k + 1, :], amount)
    twice = zeros_and_ones((experts, experts * 2), lambda d, a: a // 2 == d)
    halves = lax.broadcasted_iota(jnp.int32, (rows, experts * 2), 1) % 2
    for s in range(2):
        part = jnp.where(place == float(s), amount, 0.0).T
        high = part.astype(BF16)
        low = (part - high.astype(F32)).astype(BF16)
        for p, piece in enumerate((high, low)):
            both = nn(piece, twice)
            for h in range(2):
                rows_at = (2 * p + h) * rows
                kept_half = jnp.where(halves == h, both, 0.0).astype(BF16)
                for t in (s, s + 2):
                    combine[
                        rows_at : rows_at + rows, t * 2 * experts : (t + 1) * 2 * experts
                    ] = kept_half
    scaled = normed[...].astype(F32) * branch_gate[...].astype(F32)[None, :]
    level = jnp.sum(scaled, axis=-1, keepdims=True)
    branch[...] = jnp.broadcast_to(jax.nn.sigmoid(level), branch.shape)


STAGED = 9


def prepare_body(*refs):
    rank, bias, rate, skip, gate, up, down = refs[:7]
    proj_gate, proj_input, proj_write, proj_read, proj_step = refs[7:12]
    sources = refs[12 : 12 + STAGED]
    lanes, packed, across, along = refs[12 + STAGED : 16 + STAGED]
    targets = refs[16 + STAGED : 16 + 2 * STAGED]
    bias_here, rate_here, skip_here, built, sems = refs[16 + 2 * STAGED :]
    width, block = gate.shape
    inner = proj_gate.shape[1]
    latent = proj_write.shape[0]
    pairs = [
        (bias, bias_here),
        (rate, rate_here),
        (skip, skip_here),
    ]
    pairs += [(gate, built.at[0:width]), (up, built.at[width : 2 * width])]
    for j in range(width // block):
        first = 2 * width + j * block
        pairs.append((down.at[:, j * block : (j + 1) * block], built.at[first : first + block]))
    building = len(pairs)
    pairs += [
        (proj_gate, across.at[:, 0:inner]),
        (proj_input, across.at[:, inner : 2 * inner]),
        (proj_write, along.at[0:latent]),
        (proj_read, along.at[latent : 2 * latent]),
        (proj_step, along.at[2 * latent : 2 * latent + HEADS]),
    ]
    pairs += list(zip(sources, targets))
    copies = [pltpu.make_async_copy(a, b, sems.at[k]) for k, (a, b) in enumerate(pairs)]
    out_copy = pltpu.make_async_copy(built, packed, sems.at[len(pairs)])
    for copy in copies:
        copy.start()
    for copy in copies[:building]:
        copy.wait()
    out_copy.start()
    heads = inner // HEAD_DIM
    lane_head = lax.broadcasted_iota(jnp.int32, (1, inner), 1) // HEAD_DIM
    for k, table in enumerate((bias_here, rate_here, skip_here)):
        line = jnp.zeros((1, inner), F32)
        for h in range(heads):
            line = jnp.where(lane_head == h, table[rank[0] * heads + h], line)
        lanes[k : k + 1, :] = line
    for copy in copies[building:]:
        copy.wait()
    out_copy.wait()


def conv(window, newest, taps, out_window):
    taken = taps[...].astype(F32)
    total = newest.astype(F32) * taken[3:4]
    for k in range(3):
        total += window[k].astype(F32) * taken[k : k + 1]
    out_window[0] = window[1]
    out_window[1] = window[2]
    out_window[2] = newest
    return silu(total)


def mixer_body(
    rank,
    lanes,
    arrived,
    across,
    along,
    norm_gain,
    taps_input,
    taps_write,
    taps_read,
    input_window,
    write_window,
    read_window,
    state,
    out_gain,
    proj_out,
    partial,
    new_state,
    new_input_window,
    new_write_window,
    new_read_window,
):
    rows = arrived.shape[1]
    x = jnp.concatenate([arrived[j] for j in range(arrived.shape[0])], axis=1).astype(F32)
    scale = lax.rsqrt(jnp.mean(x * x, axis=-1, keepdims=True) + EPS)
    normed = (x * scale * norm_gain[...].astype(F32)[None, :]).astype(BF16)
    inner = input_window.shape[2]
    latent = write_window.shape[2]
    first = nn(normed, across[...])
    second = nt(normed, along[...])
    gate_rows = first[:, 0:inner].astype(BF16)
    input_rows = first[:, inner : 2 * inner].astype(BF16)
    write_rows = second[:, 0:latent].astype(BF16)
    read_rows = second[:, latent : 2 * latent].astype(BF16)
    step_all = second[:, 2 * latent : 2 * latent + HEADS]
    input_conv = conv(input_window, input_rows, taps_input, new_input_window)
    write_conv = conv(write_window, write_rows, taps_write, new_write_window)
    read_conv = conv(read_window, read_rows, taps_read, new_read_window)
    heads = inner // HEAD_DIM
    lane_head = lax.broadcasted_iota(jnp.int32, (rows, inner), 1) // HEAD_DIM
    column = lax.broadcasted_iota(jnp.int32, step_all.shape, 1)
    raw = jnp.zeros((rows, inner), F32)
    for h in range(heads):
        mine = column == rank[0] * heads + h
        raw = jnp.where(
            lane_head == h, jnp.sum(jnp.where(mine, step_all, 0.0), axis=1, keepdims=True), raw
        )
    step = softplus(raw + lanes[0:1, :])
    decay = jnp.exp(-step * lanes[1:2, :])
    scaled_t = (step * input_conv).T
    decay_t = decay.T
    lane = lax.broadcasted_iota(jnp.int32, (inner, rows), 1)
    readout_t = jnp.zeros((inner, rows), F32)
    for b in range(rows):
        fresh = (
            decay_t[:, b : b + 1] * state[b] + scaled_t[:, b : b + 1] * write_conv[b : b + 1, :]
        )
        new_state[b] = fresh
        seen = jnp.sum(fresh * read_conv[b : b + 1, :], axis=1, keepdims=True)
        readout_t = jnp.where(lane == b, seen, readout_t)
    readout = readout_t.T + lanes[2:3, :] * input_conv
    gated = readout * silu(gate_rows.astype(F32))
    gated = gated * lax.rsqrt(jnp.mean(gated * gated, axis=-1, keepdims=True) + EPS)
    mixer_rows = (gated * out_gain[...].astype(F32)[None, :]).astype(BF16)
    mixed = nn(mixer_rows, proj_out[...]).astype(BF16)
    for j in range(partial.shape[0]):
        partial[j] = mixed


def hidden_body(
    rank, arrived, mixed_in, ffn_gain, select, outgoing, normed_out, hidden_part, folded, staged, sems
):
    count, rows, quarter = arrived.shape
    pieces = folded.shape[0] // rows
    x = jnp.concatenate([arrived[j] for j in range(count)], axis=1).astype(F32)
    mixed = mixed_in[0].astype(F32)
    for j in range(1, count):
        mixed += mixed_in[j].astype(F32)
    hidden = (x + mixed).astype(BF16)
    wide = hidden.astype(F32)
    scale = lax.rsqrt(jnp.mean(wide * wide, axis=-1, keepdims=True) + EPS)
    normed_wide = wide * scale * ffn_gain[...].astype(F32)[None, :]
    normed_out[...] = normed_wide.astype(BF16)
    for j in range(pieces):
        folded[pl.ds(j, rows, stride=pieces), :] = normed_wide[:, j * 128 : (j + 1) * 128]
    lines = folded[...].astype(BF16)
    share = outgoing.shape[0] // 4
    copies = []
    for q in range(4):
        part = pl.ds(q * share, share)
        staged[part, :] = nn(select[part, :], lines).astype(BF16)
        copies.append(pltpu.make_async_copy(staged.at[part], outgoing.at[part], sems.at[q]))
        copies[q].start()
    mine = wide[:, 0:quarter]
    for j in range(1, count):
        mine = jnp.where(rank[0] == j, wide[:, j * quarter : (j + 1) * quarter], mine)
    hidden_part[...] = mine.astype(BF16)
    for copy in copies:
        copy.wait()


def dense_body(rank, normed_in, gate, up, down, give, keep):
    normed = normed_in[...]
    hidden = (silu(nn(normed, gate[...])) * nn(normed, up[...])).astype(BF16)
    total = nt(hidden, down[...]).astype(BF16)
    half = give.shape[1]
    upper = rank[0] > 1
    give[...] = jnp.where(upper, total[:, 0:half], total[:, half:])
    keep[...] = jnp.where(upper, total[:, half:], total[:, 0:half])


def halve_body(rank, keep, got, give, left):
    total = keep[...].astype(F32) + got[...].astype(F32)
    quarter = give.shape[1]
    odd = jnp.bitwise_and(rank[0], 1) > 0
    give[...] = jnp.where(odd, total[:, 0:quarter], total[:, quarter:]).astype(BF16)
    left[...] = jnp.where(odd, total[:, quarter:], total[:, 0:quarter])


def expert_body(items, gate, up, down, other, out, unfolded, fold, staged, sems):
    width, block = gate.shape
    pieces = width // 128
    count = items.shape[0] // pieces
    unfolded[...] = items[...].astype(F32)
    x = jnp.concatenate(
        [unfolded[pl.ds(j, count, stride=pieces), :].astype(BF16) for j in range(pieces)], axis=1
    )
    act = (silu(nn(x, gate[...])) * nn(x, up[...])).astype(BF16)
    act_other = (silu(nn(x, other[0:width])) * nn(x, other[width : 2 * width])).astype(BF16)
    copies = []
    for q in range(pieces // 2):
        at = q * 2 * count
        total = nn(act, down[:, 2 * q * block : 2 * (q + 1) * block])
        for h in range(2):
            first = 2 * width + (2 * q + h) * block
            piece = nn(act_other, other[first : first + block])
            piece += total[:, h * block : (h + 1) * block]
            fold[pl.ds(at + h, count, stride=2), :] = piece
        staged[at : at + 2 * count] = fold[at : at + 2 * count].astype(BF16)
        part = pl.ds(at, 2 * count)
        copies.append(pltpu.make_async_copy(staged.at[part], out.at[part], sems.at[q]))
        copies[q].start()
    for copy in copies:
        copy.wait()


def final_body(returned, combine, left, got, branch, hidden_part, out):
    total = hidden_part[...].astype(F32)
    rows = total.shape[0]
    dense = left[...] + got[...].astype(F32)
    sums = nn(combine[...], returned[...])
    sums = sums[0 : 2 * rows] + sums[2 * rows :]
    total += jnp.concatenate([sums[0:rows], sums[rows:]], axis=1)
    total += branch[:, 0:1] * dense
    out[...] = total.astype(BF16)


def local(
    tokens,
    input_window,
    write_window,
    read_window,
    ssm_state,
    norm_gain,
    proj_gate,
    proj_input,
    proj_write,
    proj_read,
    proj_step,
    taps_input,
    taps_write,
    taps_read,
    step_bias,
    decay_rate,
    skip_gain,
    out_gain,
    proj_out,
    ffn_gain,
    expert_ids,
    expert_weights,
    expert_gate,
    expert_up,
    expert_down,
    dense_gate,
    dense_up,
    dense_down,
    branch_gate,
):
    tps = lax.axis_size("tp")
    eps = lax.axis_size("ep")
    rank = lax.axis_index("tp").astype(jnp.int32).reshape(1)
    rows, quarter = tokens.shape
    width = quarter * tps
    inner = proj_gate.shape[1]
    latent = proj_write.shape[1]
    heads = ssm_state.shape[1]
    block = expert_gate.shape[2]

    pieces = width // 128

    spread = call(
        spread_body,
        sds((tps, rows, quarter), BF16),
        [HBM],
        [pltpu.VMEM((rows, quarter), BF16), pltpu.SemaphoreType.DMA((tps + 1,))],
        HBM,
    )(kept(tokens))
    arrived = lax.all_to_all(spread, "tp", 0, 0, tiled=True)

    projections = (proj_gate, proj_input, proj_write.T, proj_read.T, proj_step.T)
    staged = (
        norm_gain,
        taps_input,
        taps_write,
        taps_read,
        input_window.transpose(1, 0, 2),
        write_window.transpose(1, 0, 2),
        read_window.transpose(1, 0, 2),
        ssm_state.reshape(rows, inner, STATE),
        out_gain,
    )
    lanes, packed, *staged = call(
        prepare_body,
        (
            pltpu.VMEM((8, inner), F32),
            pltpu.HBM((3 * width, block), BF16),
            pltpu.VMEM((width, 2 * inner), BF16),
            pltpu.VMEM((2 * latent + HEADS, width), BF16),
        )
        + tuple(pltpu.VMEM(v.shape, v.dtype) for v in staged),
        [SMEM] + [HBM] * (11 + STAGED),
        [
            pltpu.SMEM(step_bias.shape, F32),
            pltpu.SMEM(step_bias.shape, F32),
            pltpu.SMEM(step_bias.shape, F32),
            pltpu.VMEM((3 * width, block), BF16),
            pltpu.SemaphoreType.DMA((11 + pieces + STAGED,)),
        ],
        (VMEM, HBM) + (VMEM,) * (2 + STAGED),
    )(
        rank,
        *map(
            kept,
            (
                step_bias,
                decay_rate,
                skip_gain,
                expert_gate[0],
                expert_up[0],
                expert_down[0],
                *projections,
                *staged,
            ),
        ),
    )

    partial, new_state, new_input, new_write, new_read = call(
        mixer_body,
        (
            pltpu.HBM((tps, rows, width), BF16),
            sds((rows, inner, STATE), F32),
            sds((3, rows, inner), BF16),
            sds((3, rows, latent), BF16),
            sds((3, rows, latent), BF16),
        ),
        [SMEM] + [VMEM] * 14,
    )(rank, lanes, arrived, *staged, proj_out)
    mixed_in = lax.all_to_all(partial, "tp", 0, 0, tiled=True)
    packed, ids, _ = lax.optimization_barrier((packed, expert_ids.T, partial))
    select = call(select_body, sds((eps * pieces, rows * pieces), BF16), [SMEM, VMEM])(rank, ids)
    other = lax.ppermute(packed, "tp", [(t, t ^ 1) for t in range(tps)])

    outgoing, normed_ffn, hidden_part = call(
        hidden_body,
        (
            pltpu.HBM((eps * pieces, 128), BF16),
            sds((rows, width), BF16),
            sds((rows, quarter), BF16),
        ),
        [SMEM] + [VMEM] * 4,
        [
            pltpu.VMEM((rows * pieces, 128), F32),
            pltpu.VMEM((eps * pieces, 128), BF16),
            pltpu.SemaphoreType.DMA((4,)),
        ],
        (HBM, VMEM, VMEM),
    )(rank, arrived, mixed_in, ffn_gain, select)
    items = lax.all_to_all(outgoing.reshape(eps, pieces, 128), "ep", 0, 0, tiled=True)

    ids, weights, gate_line, normed_ffn = lax.optimization_barrier(
        (expert_ids.T, expert_weights.T, branch_gate, normed_ffn)
    )
    combine, branch = call(
        weigh_body, (sds((4 * rows, 2 * tps * eps), BF16), sds((rows, 128), F32)), [VMEM] * 4
    )(ids, weights, normed_ffn, gate_line)
    give, keep = call(
        dense_body,
        (sds((rows, width // 2), BF16), sds((rows, width // 2), BF16)),
        [SMEM] + [VMEM] * 4,
    )(rank, normed_ffn, dense_gate, dense_up, dense_down)
    got = lax.ppermute(give, "tp", [(t, t ^ 2) for t in range(tps)])
    give, left = call(
        halve_body, (sds((rows, quarter), BF16), sds((rows, quarter), F32)), [SMEM] + [VMEM] * 2
    )(rank, keep, got)
    items, give = lax.optimization_barrier((items, give))
    got = lax.ppermute(give, "tp", [(t, t ^ 1) for t in range(tps)])

    results = call(
        expert_body,
        pltpu.HBM((tps * eps * 2, 128), BF16),
        [VMEM] * 5,
        [
            pltpu.VMEM((eps * pieces, 128), F32),
            pltpu.VMEM((tps * eps * 2, 128), F32),
            pltpu.VMEM((tps * eps * 2, 128), BF16),
            pltpu.SemaphoreType.DMA((tps,)),
        ],
        HBM,
    )(items.reshape(eps * pieces, 128), expert_gate[0], expert_up[0], expert_down[0], other)
    returned = lax.all_to_all(
        results.reshape(tps * eps, 2, 128), ("tp", "ep"), 0, 0, tiled=True
    ).reshape(tps * eps * 2, 128)

    new_hidden = call(final_body, sds((rows, quarter), BF16), [VMEM] * 6)(
        returned, combine, left, got, branch, hidden_part
    )
    return (
        new_hidden,
        new_state.reshape(rows, heads, HEAD_DIM, STATE),
        new_input.transpose(1, 0, 2),
        new_write.transpose(1, 0, 2),
        new_read.transpose(1, 0, 2),
    )


def solution(mesh):
    in_specs = (
        P("ep", "tp"),
        P("ep", None, "tp"),
        P("ep", None, "tp"),
        P("ep", None, "tp"),
        P("ep", "tp", None, None),
        P(),
        P(None, "tp"),
        P(None, "tp"),
        P(None, "tp"),
        P(None, "tp"),
        P(),
        P(None, "tp"),
        P(None, "tp"),
        P(None, "tp"),
        P(),
        P(),
        P(),
        P("tp"),
        P("tp", None),
        P(),
        P("ep", None),
        P("ep", None),
        P("ep", None, "tp"),
        P("ep", None, "tp"),
        P("ep", "tp", None),
        P(None, "tp"),
        P(None, "tp"),
        P(None, "tp"),
        P(),
    )
    out_specs = (
        P("ep", "tp"),
        P("ep", "tp", None, None),
        P("ep", None, "tp"),
        P("ep", None, "tp"),
        P("ep", None, "tp"),
    )
    return jax.shard_map(local, mesh=mesh, in_specs=in_specs, out_specs=out_specs, check_vma=False)
```
